128 devices in a mesh: ep: 64 (over z, y, x), tp: 2 (over core).
Axes of the slice: x: 4, y: 4, z: 4, core: 2. Of those that a mesh axis runs over, the one named last changes fastest.
Arguments:
- tokens: bfloat16 [3072, 2048], P('ep'), may hold values from -6 to 6
- norm_gain: bfloat16 [2048], replicated, as said below
- expert_gain: bfloat16 [2048], replicated, may hold values from 0.099609375 to 1.8984375
- w_query: bfloat16 [2048, 512], P(None, 'tp'), as said below
- key_weight: bfloat16 [2048, 256], P(None, 'tp'), may hold values from -0.125 to 0.125
- value_weight: bfloat16 [2048, 256], P(None, 'tp'), may hold values from -0.125 to 0.125
- forget_weight: bfloat16 [2048, 2], replicated, may hold values from -0.125 to 0.125
- w_out: bfloat16 [512, 2048], P('tp'), may hold values from -0.25 to 0.25
- key_cache: bfloat16 [3072, 1024, 2, 128], P('ep', None, 'tp'), may hold values from -64 to 64
- cached_values: bfloat16 [3072, 1024, 2, 128], P('ep', None, 'tp'), may hold values from -6 to 6
- cum_gates: float32 [3072, 2, 1024], P('ep', 'tp'), as said below
- lengths: int32 [3072], P('ep'), may hold values from 128 to 1024
- routes: int32 [3072, 4], P('ep'), may hold values from 0 to 63, all different within a row; in each aligned block of 48 rows (0 to 47, 48 to 95, ...) at most 6 rows name the same one
- route_weights: float32 [3072, 4], P('ep'), may hold values from 0.1 to 1
- expert_gate: bfloat16 [64, 2048, 512], P('ep', None, 'tp'), may hold values from -0.125 to 0.125
- expert_up: bfloat16 [64, 2048, 512], P('ep', None, 'tp'), may hold values from -0.125 to 0.125
- expert_down: bfloat16 [64, 512, 2048], P('ep', 'tp'), may hold values from -0.25 to 0.25
Outputs:
- hidden_out: bfloat16 [3072, 2048], P('ep', 'tp')
The draws below stay inside these ranges and needn't reach their ends.
Inputs may be any that keep to these rules, and one draw needn't show every extreme that they name: `routes`: each row names 4 different experts. Among the 48 rows of one index of ep no expert is named more than 6 times, a bound that some block reaches. `cum_gates`: entry p is the sum of the log forget values of positions 0 to p, so it never rises along the last dimension. `norm_gain`: every entry is positive and of order one. `w_query`: entries have mean zero and a spread of one over the square root of 2048.
All inputs are finite; a program needn't handle non-finite values.
Results may differ from the reference program's by a relative error of at most 0.014.
Values may be sent and summed in bfloat16 or wider, within the bound.
No kernel may reach another device: no remote copies, remote signals or barrier semaphores. Data moves between devices by JAX's collectives and lax.ppermute only.
A program may use at most 128 MiB of HBM per device.

```python
import math
import jax
import jax.numpy as jnp
import numpy as np
from jax import lax

MODEL_WIDTH = 2048
HEAD_WIDTH = 128
QUERY_HEADS = 4
KEY_VALUE_HEADS = 2
FE = 512
TOPK = 4
SEQ_DEV = 48
STORED_POSITIONS = 1024
TOKEN_COUNT = 3072
EXPERTS = 64
CAP = 6
N_EP = 64
N_TP = 2


def base_tokens(key):
    lookup_vectors = jax.random.split(jax.random.fold_in(key, 101), 1)
    return jnp.clip(jax.random.normal(lookup_vectors[0], (TOKEN_COUNT, MODEL_WIDTH), dtype=jnp.float32), -6.0, 6.0)


def base_gain(key):
    perturbation_scale = jax.random.normal(jax.random.fold_in(key, 202), (MODEL_WIDTH,), dtype=jnp.float32)
    return 1.0 + 0.18 * jnp.clip(perturbation_scale, -4.0, 4.0)


def base_query_weight(key):
    perturbation_scale = jax.random.normal(jax.random.fold_in(key, 303), (MODEL_WIDTH, QUERY_HEADS * HEAD_WIDTH), dtype=jnp.float32)
    return jnp.clip(perturbation_scale, -6.0, 6.0) * MODEL_WIDTH ** (-0.5)


def draw_tokens(key, part):
    return base_tokens(key).astype(jnp.bfloat16)


def draw_norm_gain(key, part):
    return base_gain(key).astype(jnp.bfloat16)


def draw_w_query(key, part):
    return base_query_weight(key).astype(jnp.bfloat16)


def draw_key_cache(key, part):
    tensor_dimensions = (TOKEN_COUNT, STORED_POSITIONS, KEY_VALUE_HEADS, HEAD_WIDTH)
    drawn = jnp.clip(jax.random.normal(jax.random.fold_in(key, 404), tensor_dimensions, dtype=jnp.float32), -6.0, 6.0)
    return drawn.astype(jnp.bfloat16)


def draw_cum_gates(key, part):
    lookup_vectors = jax.random.split(jax.random.fold_in(key, 17), 6)
    tensor_dimensions = (TOKEN_COUNT, KEY_VALUE_HEADS, STORED_POSITIONS)
    share_fraction = 0.5
    damping_multiplier = jax.random.uniform(lookup_vectors[0], (TOKEN_COUNT, KEY_VALUE_HEADS), dtype=jnp.float32) < share_fraction
    total_count = jax.random.uniform(lookup_vectors[1], (TOKEN_COUNT, KEY_VALUE_HEADS), dtype=jnp.float32, minval=0.3, maxval=1.0)
    quick_extent = jax.random.uniform(lookup_vectors[2], (TOKEN_COUNT, KEY_VALUE_HEADS), dtype=jnp.float32, minval=30.0, maxval=100.0)
    fading_coefficient = jnp.where(damping_multiplier, total_count / STORED_POSITIONS, 1.0 / quick_extent)
    perturbation_scale = jnp.exp(0.6 * jax.random.normal(lookup_vectors[3], tensor_dimensions, dtype=jnp.float32))
    spike_magnitude = jax.random.uniform(lookup_vectors[4], tensor_dimensions, dtype=jnp.float32) < 2.0 / STORED_POSITIONS
    layer_index = jnp.log(jax.random.uniform(lookup_vectors[5], tensor_dimensions, dtype=jnp.float32, minval=0.5, maxval=0.8))
    iteration_number = -fading_coefficient[:, :, None] * perturbation_scale + jnp.where(spike_magnitude & damping_multiplier[:, :, None], layer_index, 0.0)
    return jnp.cumsum(iteration_number, axis=-1).astype(jnp.float32)


def plant(drawn, stream_key, low, largest):
    index_at = [jax.random.randint(jax.random.fold_in(stream_key, axis), (), 0, length) for axis, length in enumerate(drawn.shape)]
    widest = drawn.shape.index(max(drawn.shape))
    beside = index_at[:widest] + [(index_at[widest] + 1) % drawn.shape[widest]] + index_at[widest + 1:]
    return drawn.at[tuple(index_at)].set(low).at[tuple(beside)].set(largest)


def level_of(key, dims, cuts, least, high):
    def one(axis_at, parts):
        draws = jax.random.uniform(jax.random.fold_in(jax.random.fold_in(key, 6), axis_at), (parts,), jnp.float32, least / len(cuts), high / len(cuts))
        return jnp.repeat(jnp.exp(draws), dims[axis_at] // parts).reshape((-1,) + (1,) * (len(dims) - axis_at - 1))

    factor_of = one(*cuts[0])
    for cut in cuts[1:]:
        factor_of = factor_of * one(*cut)
    return factor_of


def assign_block(key, own, number, rows, count, top, bound, slope):
    order = jax.random.permutation(key, count)
    heavy_load, ordinary = load_shares(count, rows * top, bound, slope, True), load_shares(count, rows * top, bound, slope, False)
    places = jnp.arange(count)

    def named(sizes, turn):
        used = int((sizes > 0).sum())
        fixed = max(1, used // 4)
        shifted = fixed + (places - fixed + turn * (used - fixed)) % max(1, count - fixed)
        return jnp.zeros((count,), jnp.int32).at[order[jnp.where(places < fixed, places, shifted)]].set(jnp.asarray(sizes, jnp.int32))

    sizes = jnp.where(number % 4 == 0, named(heavy_load, number // 4), named(ordinary, number - number // 4 - 1))
    mixed = jax.random.permutation(jax.random.fold_in(own, 3), count)
    donor, sink = mixed[0:count // 2 * 2:2], mixed[1:count // 2 * 2:2]
    slack = jnp.minimum(sizes[donor] - 1, bound - sizes[sink]) // 2
    slack = jnp.where((donor == order[0]) | (sink == order[0]) | (sizes[sink] == 0), 0, jnp.maximum(slack, 0))
    shifted = jax.random.randint(jax.random.fold_in(own, 4), (count // 2,), 0, 1 << 20) % (slack + 1)
    sizes = sizes.at[donor].add(-shifted).at[sink].add(shifted)
    labels = jnp.searchsorted(jnp.cumsum(sizes), jnp.arange(rows * top), side="right").astype(jnp.int32)
    grid = labels.reshape(top, rows).T
    grid = grid[jax.random.permutation(jax.random.fold_in(own, 1), rows)]
    turn = jax.random.randint(jax.random.fold_in(own, 2), (rows, 1), 0, top)
    return jnp.take_along_axis(grid, (jnp.arange(top)[None, :] + turn) % top, axis=1)


def load_shares(number_of, total, limit, slope, full):
    portions = [(1 << 20) // math.isqrt(standing ** slope) + 1 for standing in range(1, number_of + 1)]
    largest = limit if full else min(limit, max(-(-total // number_of), total * portions[0] // sum(portions)))
    least = 1 if total - largest >= number_of - 1 else 0
    counts, rest = [largest] + [least] * (number_of - 1), total - largest - least * (number_of - 1)
    while rest > 0:
        movable = [i for i in range(1, number_of) if counts[i] < largest] or [i for i in range(1, number_of) if counts[i] < limit]
        mass, remaining = sum([portions[i] for i in movable]), rest
        for i in movable:
            extra = min(limit - counts[i], max(1, remaining * portions[i] // mass), rest)
            counts[i] = counts[i] + extra
            rest = rest - extra
    return np.array(counts)


def normal_values(rng, shape, deviation, most, cuts=(), kind=jnp.bfloat16):
    entries = jax.random.normal(rng, shape, jnp.float32) * deviation
    if len(cuts) > 0:
        entries = level_of(rng, shape, cuts, -0.22, 0.18) * entries
    return jnp.clip(entries, min=-most, max=most).astype(kind)


def setup_inputs(seed: int = 0) -> dict:
    seeds = jax.random.split(jax.random.key(seed), 18)
    tokens = draw_tokens(jax.random.fold_in(seeds[17], 71), 0)
    norm_gain = draw_norm_gain(jax.random.fold_in(seeds[17], 71), 0)
    expert_gain = jnp.clip(1.0 + 0.18 * jax.random.normal(seeds[2], (MODEL_WIDTH,), jnp.float32), 0.099609375, 1.8984375).astype(jnp.bfloat16)
    w_query = draw_w_query(jax.random.fold_in(seeds[17], 71), 0)
    key_weight = normal_values(seeds[4], (MODEL_WIDTH, KEY_VALUE_HEADS * HEAD_WIDTH), MODEL_WIDTH ** -0.5, 0.125, ((1, 2),))
    value_weight = normal_values(seeds[5], (MODEL_WIDTH, KEY_VALUE_HEADS * HEAD_WIDTH), MODEL_WIDTH ** -0.5, 0.125, ((1, 2),))
    forget_weight = normal_values(seeds[6], (MODEL_WIDTH, KEY_VALUE_HEADS), MODEL_WIDTH ** -0.5, 0.125)
    w_out = normal_values(seeds[7], (QUERY_HEADS * HEAD_WIDTH, MODEL_WIDTH), (QUERY_HEADS * HEAD_WIDTH) ** -0.5, 0.25, ((0, 2),))
    key_cache = draw_key_cache(jax.random.fold_in(seeds[17], 71), 0)
    cached_values = normal_values(seeds[9], (TOKEN_COUNT, STORED_POSITIONS, KEY_VALUE_HEADS, HEAD_WIDTH), 1.0, 6.0, ((0, 64), (2, 2)))
    cum_gates = draw_cum_gates(jax.random.fold_in(seeds[17], 71), 0)
    lengths = plant(jax.random.randint(seeds[11], (TOKEN_COUNT,), STORED_POSITIONS // 8, STORED_POSITIONS + 1), jax.random.fold_in(seeds[11], 1), STORED_POSITIONS // 8, STORED_POSITIONS).astype(jnp.int32)
    routes_keys = jax.random.split(jax.random.fold_in(seeds[12], 1), TOKEN_COUNT // SEQ_DEV)
    routes_turns = jax.random.permutation(jax.random.fold_in(seeds[12], 3), TOKEN_COUNT // SEQ_DEV)
    routes = jax.vmap(lambda own, number: assign_block(jax.random.fold_in(seeds[12], 2), own, number, SEQ_DEV, EXPERTS, TOPK, CAP, 2))(routes_keys, routes_turns).reshape((TOKEN_COUNT, TOPK))
    route_weights = jnp.clip(0.1 + 0.9 * jax.random.uniform(seeds[13], (TOKEN_COUNT, TOPK), jnp.float32) ** level_of(seeds[13], (TOKEN_COUNT, TOPK), ((0, 64),), -0.2, 0.2), 0.1, 1.0)
    expert_gate = normal_values(seeds[14], (EXPERTS, MODEL_WIDTH, FE), MODEL_WIDTH ** -0.5, 0.125, ((0, 64), (2, 2)))
    expert_up = normal_values(seeds[15], (EXPERTS, MODEL_WIDTH, FE), MODEL_WIDTH ** -0.5, 0.125, ((0, 64), (2, 2)))
    expert_down = normal_values(seeds[16], (EXPERTS, FE, MODEL_WIDTH), FE ** -0.5, 0.25, ((0, 64), (1, 2)))
    return {"tokens": tokens, "norm_gain": norm_gain, "expert_gain": expert_gain, "w_query": w_query, "key_weight": key_weight, "value_weight": value_weight, "forget_weight": forget_weight, "w_out": w_out, "key_cache": key_cache, "cached_values": cached_values, "cum_gates": cum_gates, "lengths": lengths, "routes": routes, "route_weights": route_weights, "expert_gate": expert_gate, "expert_up": expert_up, "expert_down": expert_down}


EPS = 1e-06

def rms_rows(values, gain):
    flt = values.astype(jnp.float32)
    scale = lax.rsqrt(lax.optimization_barrier(jnp.mean(flt * flt, axis=-1, keepdims=True)) + EPS)
    return (flt * scale * gain.astype(jnp.float32)).astype(jnp.bfloat16)

def attend(query_rows, key_new, value_new, log_forget, key_cache, cached_values, cum_gates, lengths):
    seqs = key_cache.shape[0]
    kv_heads = key_cache.shape[2]
    head_size = key_cache.shape[3]
    group = query_rows.shape[1] // (kv_heads * head_size)
    scale = head_size ** (-0.5)
    q_four = query_rows.reshape(seqs, kv_heads, group, head_size)
    k_self = key_new.reshape(seqs, kv_heads, head_size)
    v_self = value_new.reshape(seqs, kv_heads, head_size)
    places = jnp.arange(key_cache.shape[1], dtype=jnp.int32)
    last = lax.optimization_barrier(jnp.sum(jnp.where(places[None, None, :] == (lengths - 1)[:, None, None], cum_gates, 0.0), axis=-1))
    bias = (log_forget + last)[:, :, None] - cum_gates
    scores = jnp.einsum('skgd,slkd->skgl', q_four.astype(jnp.float32), key_cache.astype(jnp.float32)) * scale
    scores = scores + bias[:, :, None, :]
    valid = places[None, :] < lengths[:, None]
    scores = jnp.where(valid[:, None, None, :], scores, -jnp.inf)
    own = jnp.einsum('skgd,skd->skg', q_four.astype(jnp.float32), k_self.astype(jnp.float32)) * scale
    top = jnp.maximum(lax.optimization_barrier(jnp.max(scores, axis=-1)), own)
    expo = jnp.exp(scores - top[..., None])
    own_expo = jnp.exp(own - top)
    denom = lax.optimization_barrier(jnp.sum(expo, axis=-1)) + own_expo
    probs = (expo / denom[..., None]).astype(jnp.bfloat16)
    own_prob = (own_expo / denom).astype(jnp.bfloat16)
    result = jnp.einsum('skgl,slkd->skgd', probs.astype(jnp.float32), cached_values.astype(jnp.float32))
    result = result + own_prob.astype(jnp.float32)[..., None] * v_self.astype(jnp.float32)[:, :, None, :]
    return result.astype(jnp.bfloat16).reshape(seqs, kv_heads * group * head_size)

def reference(tokens, norm_gain, expert_gain, w_query, key_weight, value_weight, forget_weight, w_out, key_cache, cached_values, cum_gates, lengths, routes, route_weights, expert_gate, expert_up, expert_down):
    normed = rms_rows(tokens, norm_gain)
    query_rows = jnp.dot(normed, w_query, preferred_element_type=jnp.float32).astype(jnp.bfloat16)
    key_new = jnp.dot(normed, key_weight, preferred_element_type=jnp.float32).astype(jnp.bfloat16)
    value_new = jnp.dot(normed, value_weight, preferred_element_type=jnp.float32).astype(jnp.bfloat16)
    log_forget = jax.nn.log_sigmoid(jnp.dot(normed, forget_weight, preferred_element_type=jnp.float32))

    def split(arr):
        return arr.reshape((N_EP, SEQ_DEV) + arr.shape[1:])

    def one_block(items):
        return attend(*items)
    attended = lax.map(one_block, tuple((split(a) for a in (query_rows, key_new, value_new, log_forget, key_cache, cached_values, cum_gates, lengths))))
    attended = attended.reshape(TOKEN_COUNT, QUERY_HEADS * HEAD_WIDTH)
    block_rows = QUERY_HEADS * HEAD_WIDTH // N_TP
    mixed = jnp.zeros((TOKEN_COUNT, MODEL_WIDTH), jnp.float32)
    for index in range(N_TP):
        part = jnp.dot(attended[:, index * block_rows:(index + 1) * block_rows], w_out[index * block_rows:(index + 1) * block_rows], preferred_element_type=jnp.float32)
        mixed = mixed + part.astype(jnp.bfloat16).astype(jnp.float32)
    resid = (tokens.astype(jnp.float32) + mixed).astype(jnp.bfloat16)
    expert_in = rms_rows(resid, expert_gain)
    flat = routes.reshape(-1)
    onehot = (flat[:, None] == jnp.arange(EXPERTS, dtype=jnp.int32)[None, :]).astype(jnp.int32)
    onehot = onehot.reshape(N_EP, SEQ_DEV * TOPK, EXPERTS)
    rank = lax.optimization_barrier(jnp.sum((jnp.cumsum(onehot, axis=1) - onehot) * onehot, axis=-1)).reshape(-1)
    source = jnp.arange(TOKEN_COUNT * TOPK, dtype=jnp.int32) // (SEQ_DEV * TOPK)
    repeated = jnp.repeat(expert_in, TOPK, axis=0)
    buffer = jnp.zeros((EXPERTS, N_EP, CAP, MODEL_WIDTH), jnp.bfloat16).at[flat, source, rank].set(repeated)
    hidden_rows = FE // N_TP

    def one_expert(items):
        rows, gate_w, up_w, down_w = items
        rows = rows.reshape(N_EP * CAP, MODEL_WIDTH)
        gate = jnp.dot(rows, gate_w, preferred_element_type=jnp.float32)
        upper = jnp.dot(rows, up_w, preferred_element_type=jnp.float32)
        act = (jax.nn.silu(gate) * upper).astype(jnp.bfloat16)
        total_count = jnp.zeros((N_EP * CAP, MODEL_WIDTH), jnp.float32)
        for index in range(N_TP):
            part = jnp.dot(act[:, index * hidden_rows:(index + 1) * hidden_rows], down_w[index * hidden_rows:(index + 1) * hidden_rows], preferred_element_type=jnp.float32)
            total_count = total_count + part.astype(jnp.bfloat16).astype(jnp.float32)
        return total_count.astype(jnp.bfloat16).reshape(N_EP, CAP, MODEL_WIDTH)
    expert_out = lax.map(one_expert, (buffer, expert_gate, expert_up, expert_down))
    picked = expert_out[flat, source, rank].astype(jnp.float32).reshape(TOKEN_COUNT, TOPK, MODEL_WIDTH)
    moe = lax.optimization_barrier(jnp.sum(picked * route_weights[:, :, None], axis=1))
    return (resid.astype(jnp.float32) + moe).astype(jnp.bfloat16)
```

```python
import jax
import jax.numpy as jnp
from jax import lax
from jax.sharding import PartitionSpec as P

EPS = 1e-06


def rms_rows(values, gain):
    flt = values.astype(jnp.float32)
    scale = lax.rsqrt(jnp.mean(flt * flt, axis=-1, keepdims=True) + EPS)
    return (flt * scale * gain.astype(jnp.float32)).astype(jnp.bfloat16)


def attend(
    query_rows, key_new, value_new, log_forget, key_cache, cached_values, cum_gates, lengths
):
    seqs = key_cache.shape[0]
    kv_heads = key_cache.shape[2]
    head_size = key_cache.shape[3]
    group = query_rows.shape[1] // (kv_heads * head_size)
    scale = head_size ** (-0.5)
    q_four = query_rows.reshape(seqs, kv_heads, group, head_size)
    k_self = key_new.reshape(seqs, kv_heads, head_size)
    v_self = value_new.reshape(seqs, kv_heads, head_size)
    places = jnp.arange(key_cache.shape[1], dtype=jnp.int32)
    last = jnp.sum(
        jnp.where(places[None, None, :] == (lengths - 1)[:, None, None], cum_gates, 0.0), axis=-1
    )
    bias = (log_forget + last)[:, :, None] - cum_gates
    scores = (
        jnp.einsum("skgd,slkd->skgl", q_four, key_cache, preferred_element_type=jnp.float32) * scale
    )
    scores = scores + bias[:, :, None, :]
    valid = places[None, :] < lengths[:, None]
    scores = jnp.where(valid[:, None, None, :], scores, -jnp.inf)
    own = jnp.einsum("skgd,skd->skg", q_four, k_self, preferred_element_type=jnp.float32) * scale
    top = jnp.maximum(jnp.max(scores, axis=-1), own)
    expo = jnp.exp(scores - top[..., None])
    own_expo = jnp.exp(own - top)
    denom = jnp.sum(expo, axis=-1) + own_expo
    probs = (expo / denom[..., None]).astype(jnp.bfloat16)
    own_prob = (own_expo / denom).astype(jnp.bfloat16)
    result = jnp.einsum("skgl,slkd->skgd", probs, cached_values, preferred_element_type=jnp.float32)
    result = (
        result + own_prob.astype(jnp.float32)[..., None] * v_self.astype(jnp.float32)[:, :, None, :]
    )
    return result.astype(jnp.bfloat16).reshape(seqs, kv_heads * group * head_size)


def shards(
    tokens,
    norm_gain,
    expert_gain,
    w_query,
    key_weight,
    value_weight,
    forget_weight,
    w_out,
    key_cache,
    cached_values,
    cum_gates,
    lengths,
    routes,
    route_weights,
    expert_gate,
    expert_up,
    expert_down,
):
    seqs, width = tokens.shape
    n_ep = lax.axis_size("ep")
    kv_loc = key_cache.shape[2]
    normed = rms_rows(tokens, norm_gain)
    forget_cols = lax.dynamic_slice_in_dim(forget_weight, lax.axis_index("tp") * kv_loc, kv_loc, 1)
    log_forget = jax.nn.log_sigmoid(
        jnp.dot(normed, forget_cols, preferred_element_type=jnp.float32)
    )
    query_rows = jnp.dot(normed, w_query, preferred_element_type=jnp.float32).astype(jnp.bfloat16)
    key_new = jnp.dot(normed, key_weight, preferred_element_type=jnp.float32).astype(jnp.bfloat16)
    value_new = jnp.dot(normed, value_weight, preferred_element_type=jnp.float32).astype(
        jnp.bfloat16
    )
    attended = attend(
        query_rows, key_new, value_new, log_forget, key_cache, cached_values, cum_gates, lengths
    )
    swap = [(0, 1), (1, 0)]
    core = lax.axis_index("tp")
    partial_out = jnp.dot(attended, w_out, preferred_element_type=jnp.float32).astype(jnp.bfloat16)
    other_out = lax.ppermute(partial_out, "tp", swap)
    mixed = partial_out.astype(jnp.float32) + other_out.astype(jnp.float32)
    resid = (tokens.astype(jnp.float32) + mixed).astype(jnp.bfloat16)
    expert_in = rms_rows(resid, expert_gain)
    topk = routes.shape[1]
    n_exp = expert_gate.shape[0] * n_ep
    cap = max(2, 2 * seqs * topk // n_exp)
    share = cap // 2
    gate_own, up_own, down_own = expert_gate[0], expert_up[0], expert_down[0]
    gate_peer, up_peer, down_peer = (
        lax.ppermute(w, "tp", swap) for w in (gate_own, up_own, down_own)
    )
    flat = routes.reshape(-1)
    order = jnp.arange(flat.shape[0], dtype=jnp.int32)
    earlier = (flat[:, None] == flat[None, :]) & (order[None, :] < order[:, None])
    rank = jnp.sum(earlier.astype(jnp.int32), axis=-1) - core * share
    slot = jnp.where((rank >= 0) & (rank < share), flat * share + rank, -1)
    dispatch = (jnp.arange(n_exp * share, dtype=jnp.int32)[:, None] == slot[None, :]).astype(
        jnp.bfloat16
    )
    repeated = jnp.repeat(expert_in, topk, axis=0)
    send = jnp.dot(dispatch, repeated, preferred_element_type=jnp.float32).astype(jnp.bfloat16)
    send = send.reshape(n_exp, share * width // 128, 128)
    received = lax.all_to_all(send, "ep", split_axis=0, concat_axis=0, tiled=True)
    rows = received.reshape(n_exp * share, width)

    def hidden(gate_w, up_w):
        gate = jnp.dot(rows, gate_w, preferred_element_type=jnp.float32)
        upper = jnp.dot(rows, up_w, preferred_element_type=jnp.float32)
        return (jax.nn.silu(gate) * upper).astype(jnp.bfloat16)

    outputs = jnp.dot(
        hidden(gate_own, up_own), down_own, preferred_element_type=jnp.float32
    ) + jnp.dot(hidden(gate_peer, up_peer), down_peer, preferred_element_type=jnp.float32)
    outputs = outputs.astype(jnp.bfloat16).reshape(n_exp, share * width // 128, 128)
    returned = lax.all_to_all(outputs, "ep", split_axis=0, concat_axis=0, tiled=True)
    picked = jnp.dot(
        dispatch.T, returned.reshape(n_exp * share, width), preferred_element_type=jnp.float32
    )
    moe = jnp.sum(picked.reshape(seqs, topk, width) * route_weights[:, :, None], axis=1)
    half = width // 2
    keep = lax.dynamic_slice_in_dim(moe, core * half, half, 1)
    give = lax.dynamic_slice_in_dim(moe, (1 - core) * half, half, 1)
    got = lax.ppermute(give, "tp", swap)
    resid_half = lax.dynamic_slice_in_dim(resid.astype(jnp.float32), core * half, half, 1)
    return (resid_half + (keep + got)).astype(jnp.bfloat16)


def solution(mesh):
    in_specs = (
        P("ep", None),
        P(),
        P(),
        P(None, "tp"),
        P(None, "tp"),
        P(None, "tp"),
        P(),
        P("tp", None),
        P("ep", None, "tp", None),
        P("ep", None, "tp", None),
        P("ep", "tp", None),
        P("ep"),
        P("ep", None),
        P("ep", None),
        P("ep", None, "tp"),
        P("ep", None, "tp"),
        P("ep", "tp", None),
    )
    out_specs = P("ep", "tp")
    return jax.shard_map(shards, mesh=mesh, in_specs=in_specs, out_specs=out_specs, check_vma=False)
```

```python
import functools
import jax
import jax.numpy as jnp
from jax import lax
from jax.experimental import pallas as pl
from jax.experimental.pallas import tpu as pltpu
from jax.sharding import PartitionSpec as P

EPS = 1e-06
LANES = 128
GROUP = 8
F32, BF16 = jnp.float32, jnp.bfloat16


def dot(a, b):
    return jnp.dot(a, b, preferred_element_type=F32)


def dot_nt(a, b):
    return lax.dot_general(a, b, (((1,), (1,)), ((), ())), preferred_element_type=F32)


def scaled_rows(flt, gain):
    scale = lax.rsqrt(jnp.mean(flt * flt, axis=-1, keepdims=True) + EPS)
    blocks = [
        flt[:, j * LANES : (j + 1) * LANES] * scale * gain[j : j + 1, :]
        for j in range(gain.shape[0])
    ]
    return jnp.concatenate(blocks, axis=1).astype(BF16)


def attention_kernel(
    share, lengths, core, tokens_hbm, gain_hbm, wq_hbm, wk_hbm, wv_hbm, forget_hbm, wo_hbm,
    keys_hbm, values_hbm, gates_hbm, routes_hbm, partial_ref, slots_ref,
    tokens, gain, wq, wk, wv, forget, wo, keys, values, gates, routes, attended,
    small_sems, key_sems, value_sems,
):
    seqs, places, head = keys.shape
    small = [
        (tokens_hbm, tokens), (gain_hbm, gain), (wq_hbm, wq), (wk_hbm, wk), (wv_hbm, wv),
        (forget_hbm, forget), (gates_hbm, gates), (routes_hbm, routes), (wo_hbm, wo),
    ]
    copies = [pltpu.make_async_copy(a, b, small_sems.at[i]) for i, (a, b) in enumerate(small)]

    def cached(hbm, vmem, sems, s):
        filled = pl.multiple_of((lengths[s] + LANES - 1) // LANES * LANES, LANES)
        return pltpu.make_async_copy(
            hbm.at[s, pl.ds(0, filled)], vmem.at[s, pl.ds(0, filled)], sems.at[s]
        )

    for c in copies[:-1]:
        c.start()
    groups = seqs // GROUP

    def each(action, hbm, vmem, sems, g):
        for s in range(g * GROUP, (g + 1) * GROUP):
            getattr(cached(hbm, vmem, sems, s), action)()

    each("start", keys_hbm, keys, key_sems, 0)
    each("start", keys_hbm, keys, key_sems, 1)

    def clear(s, _):
        values[s] = jnp.zeros((places, head), BF16)
        return 0

    lax.fori_loop(0, seqs, clear, 0)
    for g in range(groups):
        each("start", values_hbm, values, value_sems, g)
        if g + 2 < groups:
            each("start", keys_hbm, keys, key_sems, g + 2)
    copies[-1].start()
    for c in copies[:-1]:
        c.wait()

    named = routes[...]
    top, n_exp = named.shape[0], 64
    expert = lax.broadcasted_iota(jnp.int32, (n_exp, seqs), 0)
    hits = [expert == named[k : k + 1, :] for k in range(top)]
    onehot = sum(h.astype(F32) for h in hits)
    before = lax.broadcasted_iota(jnp.int32, (seqs, seqs), 0) < lax.broadcasted_iota(
        jnp.int32, (seqs, seqs), 1
    )
    count = dot(onehot.astype(BF16), before.astype(BF16))
    for k in range(top):
        rank = jnp.sum(jnp.where(hits[k], count, 0.0), axis=0, keepdims=True).astype(jnp.int32)
        rank = rank - core[0] * share
        mine = (rank >= 0) & (rank < share)
        slots_ref[k : k + 1, :] = jnp.where(mine, named[k : k + 1, :] * share + rank, -1)

    normed = scaled_rows(tokens[...].astype(F32), gain[...].astype(F32))
    query = dot(normed, wq[...]).astype(BF16)
    key_new = dot(normed, wk[...]).astype(BF16).astype(F32)
    value_new = dot(normed, wv[...]).astype(BF16).astype(F32)
    raw = dot_nt(normed, forget[...])
    column = lax.broadcasted_iota(jnp.int32, raw.shape, 1) == core[0]
    raw = jnp.sum(jnp.where(column, raw, 0.0), axis=1, keepdims=True)
    log_forget = jnp.minimum(raw, 0.0) - jnp.log1p(jnp.exp(-jnp.abs(raw)))

    scale = head ** (-0.5)
    rows2 = lax.broadcasted_iota(jnp.int32, (2 * GROUP, 1), 0) % GROUP
    rows1 = lax.broadcasted_iota(jnp.int32, (GROUP, 1), 0)
    place = lax.broadcasted_iota(jnp.int32, (GROUP, places), 1)

    def scores_of(g):
        own_rows = slice(g * GROUP, (g + 1) * GROUP)
        q_two = jnp.concatenate([query[own_rows, :head], query[own_rows, head:]], axis=0)
        raw_scores = jnp.zeros((2 * GROUP, places), F32)
        for i in range(GROUP):
            raw_scores = jnp.where(
                rows2 == i, dot_nt(q_two, keys[g * GROUP + i]), raw_scores
            )
        return q_two, raw_scores

    def probs_of(g, q_two, raw_scores):
        own_rows = slice(g * GROUP, (g + 1) * GROUP)
        size = jnp.zeros((GROUP, 1), jnp.int32)
        for i in range(GROUP):
            size = jnp.where(rows1 == i, lengths[g * GROUP + i], size)
        steps = places // LANES
        cum = jnp.concatenate(
            [gates[pl.ds(g * GROUP * steps + j, GROUP, stride=steps), :] for j in range(steps)],
            axis=1,
        )
        last = jnp.sum(jnp.where(place == size - 1, cum, 0.0), axis=1, keepdims=True)
        bias = (log_forget[own_rows] + last) - cum
        valid = place < size
        both = jnp.concatenate([bias, bias], axis=0)
        keep = jnp.concatenate([size, size], axis=0)
        scores = raw_scores * scale + both
        place2 = lax.broadcasted_iota(jnp.int32, (2 * GROUP, places), 1)
        scores = jnp.where(place2 < keep, scores, -jnp.inf)
        k_two = jnp.concatenate([key_new[own_rows], key_new[own_rows]], axis=0)
        own = jnp.sum(q_two.astype(F32) * k_two, axis=1, keepdims=True) * scale
        peak = jnp.maximum(jnp.max(scores, axis=1, keepdims=True), own)
        expo = jnp.exp(scores - peak)
        own_expo = jnp.exp(own - peak)
        denom = jnp.sum(expo, axis=1, keepdims=True) + own_expo
        inverse = 1.0 / denom
        probs = (expo * inverse).astype(BF16)
        own_prob = (own_expo * inverse).astype(BF16).astype(F32)
        v_two = jnp.concatenate([value_new[own_rows], value_new[own_rows]], axis=0)
        return probs, own_prob * v_two

    def result_of(g, probs, own):
        result = jnp.zeros((2 * GROUP, head), F32)
        for i in range(GROUP):
            result = jnp.where(rows2 == i, dot(probs, values[g * GROUP + i]), result)
        result = (result + own).astype(BF16)
        own_rows = slice(g * GROUP, (g + 1) * GROUP)
        attended[own_rows, :head] = result[:GROUP]
        attended[own_rows, head:] = result[GROUP:]

    each("wait", keys_hbm, keys, key_sems, 0)
    pending = scores_of(0)
    for g in range(groups):
        each("wait", values_hbm, values, value_sems, g)
        if g + 1 < groups:
            each("wait", keys_hbm, keys, key_sems, g + 1)
        probs, own = probs_of(g, *pending)
        if g + 1 < groups:
            pending = scores_of(g + 1)
        result_of(g, probs, own)
    copies[-1].wait()
    partial_ref[...] = dot(attended[...], wo[...]).astype(BF16)


def attention(share, tokens, gain, wq, wk, wv, forget, wo, keys, values, gates, lengths, routes, core):
    seqs, places, head = keys.shape
    anywhere = pl.BlockSpec(memory_space=pl.ANY)
    scalar = pl.BlockSpec(memory_space=pltpu.SMEM)
    inputs = (tokens, gain, wq, wk, wv, forget, wo, keys, values, gates, routes)
    order = (tokens, gain, wq, wk, wv, forget, wo, keys, values, gates, routes)
    return pl.pallas_call(
        functools.partial(attention_kernel, share),
        out_shape=(
            jax.ShapeDtypeStruct(tokens.shape, BF16),
            jax.ShapeDtypeStruct(routes.shape, jnp.int32),
        ),
        in_specs=[scalar, scalar] + [anywhere] * len(inputs),
        out_specs=(pl.BlockSpec(memory_space=pltpu.VMEM), pl.BlockSpec(memory_space=pltpu.VMEM)),
        scratch_shapes=[pltpu.VMEM(a.shape, a.dtype) for a in order]
        + [
            pltpu.VMEM((seqs, wo.shape[0]), BF16),
            pltpu.SemaphoreType.DMA((9,)),
            pltpu.SemaphoreType.DMA((seqs,)),
            pltpu.SemaphoreType.DMA((seqs,)),
        ],
        compiler_params=pltpu.CompilerParams(vmem_limit_bytes=56 << 20),
        name="attention",
    )(lengths, core, *inputs)


def dispatch_kernel(
    tokens_ref, own_ref, peer_ref, gain_ref, slots_any, send_ref, resid_ref, wide, rows, slots, sem
):
    top, seqs = slots.shape
    copy = pltpu.make_async_copy(slots_any, slots, sem)
    copy.start()
    mixed = own_ref[...].astype(F32) + peer_ref[...].astype(F32)
    resid = (tokens_ref[...].astype(F32) + mixed).astype(BF16)
    resid_ref[...] = resid
    expert_in = scaled_rows(resid.astype(F32), gain_ref[...].astype(F32)).astype(F32)
    for j in range(wide.shape[1]):
        wide[:, j, :] = expert_in[:, j * LANES : (j + 1) * LANES]
    used = send_ref.shape[0]
    copy.wait()
    for t in range(seqs):
        row = wide[t].astype(BF16)
        for k in range(top):
            slot = slots[k, t]
            rows[jnp.where(slot < 0, used, slot)] = row
    send_ref[...] = rows[:used]


def dispatch(used, tokens, own, peer, gain, slots):
    seqs, width = tokens.shape
    blocks = width // LANES
    vmem = pl.BlockSpec(memory_space=pltpu.VMEM)
    return pl.pallas_call(
        dispatch_kernel,
        out_shape=(
            pltpu.VMEM((used, blocks, LANES), BF16),
            pltpu.VMEM((seqs, width), BF16),
        ),
        in_specs=[vmem] * 4 + [SLOTS_SPEC],
        out_specs=(vmem, vmem),
        scratch_shapes=[
            pltpu.VMEM((seqs, blocks, LANES), F32),
            pltpu.VMEM((used + 8, blocks, LANES), BF16),
            pltpu.SMEM(slots.shape, jnp.int32),
            pltpu.SemaphoreType.DMA,
        ],
        name="dispatch",
    )(tokens, own, peer, gain, slots)


def experts_kernel(
    rows_ref, gate_own, up_own, down_own, gate_peer, up_peer, down_peer, out_ref, wide
):
    blocks = wide.shape[1]
    wide[...] = rows_ref[...].astype(F32)
    rows = jnp.concatenate([wide[:, j, :].astype(BF16) for j in range(blocks)], axis=1)

    def hidden(gate_w, up_w):
        gate = dot(rows, gate_w[...])
        return (gate / (1.0 + jnp.exp(-gate)) * dot(rows, up_w[...])).astype(BF16)

    act = jnp.concatenate([hidden(gate_own, up_own), hidden(gate_peer, up_peer)], axis=1)
    down = jnp.concatenate([down_own[...], down_peer[...]], axis=0)
    outputs = dot(act, down)
    for j in range(blocks):
        wide[:, j, :] = outputs[:, j * LANES : (j + 1) * LANES]
    out_ref[...] = wide[...].astype(BF16)


def experts(rows, *weights):
    vmem = pl.BlockSpec(memory_space=pltpu.VMEM)
    return pl.pallas_call(
        experts_kernel,
        out_shape=pltpu.VMEM(rows.shape, BF16),
        in_specs=[vmem] * 7,
        out_specs=vmem,
        scratch_shapes=[pltpu.VMEM(rows.shape, F32)],
        compiler_params=pltpu.CompilerParams(vmem_limit_bytes=40 << 20),
        name="experts",
    )(rows, *weights)


def combine_kernel(
    core, shares_any, slots_any, returned_ref, resid_ref, keep_ref, give_ref, wide, shares, slots, sems
):
    top, seqs = slots.shape
    copies = [
        pltpu.make_async_copy(slots_any, slots, sems.at[0]),
        pltpu.make_async_copy(shares_any, shares, sems.at[1]),
    ]
    for c in copies:
        c.start()
    for c in copies:
        c.wait()
    for t in range(seqs):
        total = jnp.zeros(wide.shape[1:], F32)
        for k in range(top):
            slot = slots[k, t]
            row = returned_ref[jnp.maximum(slot, 0)].astype(F32)
            total = total + jnp.where(slot >= 0, row * shares[k, t], 0.0)
        wide[t] = total
    half = wide.shape[1] // 2
    width = half * LANES
    mine = core[0]

    def columns(which):
        return jnp.concatenate([wide[:, which * half + j, :] for j in range(half)], axis=1)

    resid = jnp.where(mine == 0, resid_ref[:, :width], resid_ref[:, width:])
    keep_ref[...] = columns(mine) + resid.astype(F32)
    give_ref[...] = columns(1 - mine)


def combine(returned, slots, shares, resid, core):
    seqs, width = resid.shape
    blocks = width // LANES
    vmem = pl.BlockSpec(memory_space=pltpu.VMEM)
    half = pltpu.VMEM((seqs, width // 2), F32)
    return pl.pallas_call(
        combine_kernel,
        out_shape=(half, half),
        in_specs=[pl.BlockSpec(memory_space=pltpu.SMEM), SLOTS_SPEC, SLOTS_SPEC, vmem, vmem],
        out_specs=(vmem, vmem),
        scratch_shapes=[
            pltpu.VMEM((seqs, blocks, LANES), F32),
            pltpu.SMEM(shares.shape, F32),
            pltpu.SMEM(slots.shape, jnp.int32),
            pltpu.SemaphoreType.DMA((2,)),
        ],
        name="combine",
    )(core, shares, slots, returned, resid)


SLOTS_SPEC = pl.BlockSpec(memory_space=pl.ANY)


def shards(
    tokens, norm_gain, expert_gain, w_query, key_weight, value_weight, forget_weight, w_out,
    key_cache, cached_values, cum_gates, lengths, routes, route_weights, expert_gate, expert_up,
    expert_down,
):
    seqs, width = tokens.shape
    places, head = key_cache.shape[1], key_cache.shape[3]
    n_exp = expert_gate.shape[0] * lax.axis_size("ep")
    share = max(2, 2 * seqs * routes.shape[1] // n_exp) // 2
    used, blocks = n_exp * share, width // LANES
    swap = [(0, 1), (1, 0)]
    core = lax.axis_index("tp").reshape(1)
    own, slots = attention(
        share, tokens, norm_gain.reshape(blocks, LANES), w_query, key_weight, value_weight,
        forget_weight.T, w_out, key_cache.reshape(seqs, places, head),
        cached_values.reshape(seqs, places, head), cum_gates.reshape(-1, LANES), lengths,
        routes.T, core,
    )
    peer = lax.ppermute(own, "tp", swap)
    weights = (expert_gate[0], expert_up[0], expert_down[0])
    other = tuple(lax.ppermute(w, "tp", swap) for w in weights)
    send, resid = dispatch(used, tokens, own, peer, expert_gain.reshape(blocks, LANES), slots)

    def exchange(rows):
        slabs = rows.reshape(n_exp, share * blocks, LANES)
        slabs = lax.all_to_all(slabs, "ep", split_axis=0, concat_axis=0, tiled=True)
        return slabs.reshape(used, blocks, LANES)

    outputs = experts(exchange(send), *weights, *other)
    keep, give = combine(exchange(outputs), slots, route_weights.T, resid, core)
    got = lax.ppermute(give, "tp", swap)
    return (keep + got).astype(BF16)


def solution(mesh):
    in_specs = (
        P("ep", None),
        P(),
        P(),
        P(None, "tp"),
        P(None, "tp"),
        P(None, "tp"),
        P(),
        P("tp", None),
        P("ep", None, "tp", None),
        P("ep", None, "tp", None),
        P("ep", "tp", None),
        P("ep"),
        P("ep", None),
        P("ep", None),
        P("ep", None, "tp"),
        P("ep", None, "tp"),
        P("ep", "tp", None),
    )
    out_specs = P("ep", "tp")
    return jax.shard_map(shards, mesh=mesh, in_specs=in_specs, out_specs=out_specs, check_vma=False)
```

```python
import functools
import jax
import jax.numpy as jnp
from jax import lax
from jax.experimental import pallas as pl
from jax.experimental.pallas import tpu as pltpu
from jax.sharding import PartitionSpec as P

EPS = 1e-06
LANES = 128
GROUP = 8
CHUNK = 256
SPANS = ((0,),(1,),(2,),(3,),(4,),(5,))
F32, BF16 = jnp.float32, jnp.bfloat16


def dot(a, b):
    return jnp.dot(a, b, preferred_element_type=F32)


def dot_nt(a, b):
    return lax.dot_general(a, b, (((1,), (1,)), ((), ())), preferred_element_type=F32)


def scaled_rows(flt, gain):
    scale = lax.rsqrt(jnp.mean(flt * flt, axis=-1, keepdims=True) + EPS)
    blocks = [
        flt[:, j * LANES : (j + 1) * LANES] * scale * gain[j : j + 1, :]
        for j in range(gain.shape[0])
    ]
    return jnp.concatenate(blocks, axis=1).astype(BF16)


def attention_kernel(
    share, lengths, core, tokens_hbm, gain_hbm, wq_hbm, wk_hbm, wv_hbm, forget_hbm, wo_hbm,
    keys_hbm, values_hbm, gates_hbm, routes_hbm, gate_hbm, up_hbm, down_hbm, partial_ref, slots_ref,
    gate_ref, up_ref, down_ref,
    tokens, gain, wq, wk, wv, forget, wo, keys, values, gates, routes, attended,
    small_sems, key_sems, value_sems, weight_sems,
):
    seqs = attended.shape[0]
    places, head = keys.shape[0] // seqs, keys.shape[1]
    small = [
        (tokens_hbm, tokens), (gain_hbm, gain), (wq_hbm, wq), (wk_hbm, wk), (wv_hbm, wv),
        (forget_hbm, forget), (gates_hbm, gates), (routes_hbm, routes), (wo_hbm, wo),
    ]
    copies = [pltpu.make_async_copy(a, b, small_sems.at[i]) for i, (a, b) in enumerate(small)]

    def filled(s):
        return lax.shift_right_logical(lengths[s] + (LANES - 1), 7)

    def start(hbm, vmem, sems, which):
        for g in which:
            for s in range(g * GROUP, (g + 1) * GROUP):
                count = pl.multiple_of(lax.shift_left(filled(s), 7), LANES)
                at = pl.ds(s * places, count)
                pltpu.make_async_copy(hbm.at[at], vmem.at[at], sems.at[g]).start()

    def wait(hbm, vmem, sems, which):
        for g in which:
            count = sum(filled(s) for s in range(g * GROUP, (g + 1) * GROUP))
            at = pl.ds(0, pl.multiple_of(lax.shift_left(count, 7), LANES))
            pltpu.make_async_copy(hbm.at[at], vmem.at[at], sems.at[g]).wait()

    def start_values(which):
        for g in which:
            for s in range(g * GROUP, (g + 1) * GROUP):
                edge = jnp.minimum(filled(s), places // LANES - 1)
                at = pl.multiple_of(s * places + lax.shift_left(edge, 7), LANES)
                values[pl.ds(at, LANES), :] = jnp.zeros((LANES, head), BF16)
        start(values_hbm, values, value_sems, which)

    for c in copies[:-1]:
        c.start()
    spans = SPANS + ((), (), ())
    start(keys_hbm, keys, key_sems, spans[0])
    for c in copies[:-1]:
        c.wait()
    start(keys_hbm, keys, key_sems, spans[1])
    start_values(spans[0])
    start(keys_hbm, keys, key_sems, spans[2])
    start_values(spans[1])
    copies[-1].start()

    named = routes[...]
    top, n_exp = named.shape[0], 64
    expert = lax.broadcasted_iota(jnp.int32, (n_exp, seqs), 0)
    hits = [expert == named[k : k + 1, :] for k in range(top)]
    onehot = sum(h.astype(F32) for h in hits)
    before = lax.broadcasted_iota(jnp.int32, (seqs, seqs), 0) < lax.broadcasted_iota(
        jnp.int32, (seqs, seqs), 1
    )
    count = dot(onehot.astype(BF16), before.astype(BF16))
    for k in range(top):
        rank = jnp.sum(jnp.where(hits[k], count, 0.0), axis=0, keepdims=True).astype(jnp.int32)
        rank = rank - core[0] * share
        mine = (rank >= 0) & (rank < share)
        slots_ref[k : k + 1, :] = jnp.where(mine, named[k : k + 1, :] * share + rank, -1)

    normed = scaled_rows(tokens[...].astype(F32), gain[...].astype(F32))
    query = dot(normed, wq[...]).astype(BF16)
    key_new = dot(normed, wk[...]).astype(BF16).astype(F32)
    value_new = dot(normed, wv[...]).astype(BF16).astype(F32)
    raw = dot_nt(normed, forget[...])
    column = lax.broadcasted_iota(jnp.int32, raw.shape, 1) == core[0]
    raw = jnp.sum(jnp.where(column, raw, 0.0), axis=1, keepdims=True)
    log_forget = jnp.minimum(raw, 0.0) - jnp.log1p(jnp.exp(-jnp.abs(raw)))

    scale = head ** (-0.5)
    rows2 = lax.broadcasted_iota(jnp.int32, (2 * GROUP, 1), 0) % GROUP
    rows1 = lax.broadcasted_iota(jnp.int32, (GROUP, 1), 0)
    place = lax.broadcasted_iota(jnp.int32, (GROUP, places), 1)

    def scores_of(g):
        own_rows = slice(g * GROUP, (g + 1) * GROUP)
        q_two = jnp.concatenate([query[own_rows, :head], query[own_rows, head:]], axis=0)
        raw_scores = jnp.zeros((2 * GROUP, places), F32)
        for i in range(GROUP):
            raw_scores = jnp.where(
                rows2 == i, dot_nt(q_two, keys[(g * GROUP + i) * places : (g * GROUP + i + 1) * places]), raw_scores
            )
        return q_two, raw_scores

    def probs_of(g, q_two, raw_scores):
        own_rows = slice(g * GROUP, (g + 1) * GROUP)
        size = jnp.zeros((GROUP, 1), jnp.int32)
        for i in range(GROUP):
            size = jnp.where(rows1 == i, lengths[g * GROUP + i], size)
        steps = places // LANES
        cum = jnp.concatenate(
            [gates[pl.ds(g * GROUP * steps + j, GROUP, stride=steps), :] for j in range(steps)],
            axis=1,
        )
        last = jnp.sum(jnp.where(place == size - 1, cum, 0.0), axis=1, keepdims=True)
        bias = (log_forget[own_rows] + last) - cum
        valid = place < size
        both = jnp.concatenate([bias, bias], axis=0)
        keep = jnp.concatenate([size, size], axis=0)
        scores = raw_scores * scale + both
        place2 = lax.broadcasted_iota(jnp.int32, (2 * GROUP, places), 1)
        scores = jnp.where(place2 < keep, scores, -jnp.inf)
        k_two = jnp.concatenate([key_new[own_rows], key_new[own_rows]], axis=0)
        own = jnp.sum(q_two.astype(F32) * k_two, axis=1, keepdims=True) * scale
        peak = jnp.maximum(jnp.max(scores, axis=1, keepdims=True), own)
        expo = jnp.exp(scores - peak)
        own_expo = jnp.exp(own - peak)
        denom = jnp.sum(expo, axis=1, keepdims=True) + own_expo
        inverse = 1.0 / denom
        probs = (expo * inverse).astype(BF16)
        own_prob = (own_expo * inverse).astype(BF16).astype(F32)
        v_two = jnp.concatenate([value_new[own_rows], value_new[own_rows]], axis=0)
        return probs, own_prob * v_two

    def result_of(g, probs, own):
        result = own
        for i in range(GROUP):
            s = g * GROUP + i
            for c in range(0, places, CHUNK):
                part = dot(probs[:, c : c + CHUNK], values[s * places + c : s * places + c + CHUNK])
                used = rows2 == i
                if c:
                    used = used & (lengths[s] > c)
                result = result + jnp.where(used, part, 0.0)
        result = result.astype(BF16)
        own_rows = slice(g * GROUP, (g + 1) * GROUP)
        attended[own_rows, :head] = result[:GROUP]
        attended[own_rows, head:] = result[GROUP:]

    wait(keys_hbm, keys, key_sems, spans[0])
    pairs = [(gate_hbm, gate_ref), (up_hbm, up_ref), (down_hbm, down_ref)]
    moved = [pltpu.make_async_copy(a, b, weight_sems.at[i]) for i, (a, b) in enumerate(pairs)]
    pending = [scores_of(g) for g in spans[0]]
    for i, span in enumerate(SPANS):
        start(keys_hbm, keys, key_sems, spans[i + 3])
        start_values(spans[i + 2])
        if i + 3 == len(SPANS):
            for c in moved:
                c.start()
        wait(values_hbm, values, value_sems, span)
        wait(keys_hbm, keys, key_sems, spans[i + 1])
        ready = [probs_of(g, *p) for g, p in zip(span, pending)]
        pending = [scores_of(g) for g in spans[i + 1]]
        for g, (probs, own) in zip(span, ready):
            result_of(g, probs, own)
    for c in moved:
        c.wait()
    copies[-1].wait()
    partial_ref[...] = dot(attended[...], wo[...]).astype(BF16)


def attention(
    share, tokens, gain, wq, wk, wv, forget, wo, keys, values, gates, lengths, routes, core, weights
):
    seqs = tokens.shape[0]
    anywhere = pl.BlockSpec(memory_space=pl.ANY)
    hbm = pl.BlockSpec(memory_space=pltpu.HBM)
    scalar = pl.BlockSpec(memory_space=pltpu.SMEM)
    inputs = (tokens, gain, wq, wk, wv, forget, wo, keys, values, gates, routes)
    order = (tokens, gain, wq, wk, wv, forget, wo, keys, values, gates, routes)
    return pl.pallas_call(
        functools.partial(attention_kernel, share),
        out_shape=(
            pltpu.VMEM(tokens.shape, BF16),
            pltpu.VMEM(routes.shape, jnp.int32),
            *(pltpu.VMEM(w.shape, w.dtype) for w in weights),
        ),
        in_specs=[scalar, scalar] + [anywhere] * len(inputs) + [hbm] * len(weights),
        out_specs=[pl.BlockSpec(memory_space=pltpu.VMEM)] * (2 + len(weights)),
        scratch_shapes=[pltpu.VMEM(a.shape, a.dtype) for a in order]
        + [
            pltpu.VMEM((seqs, wo.shape[0]), BF16),
            pltpu.SemaphoreType.DMA((9,)),
            pltpu.SemaphoreType.DMA((seqs // GROUP,)),
            pltpu.SemaphoreType.DMA((seqs // GROUP,)),
            pltpu.SemaphoreType.DMA((len(weights),)),
        ],
        compiler_params=pltpu.CompilerParams(vmem_limit_bytes=52 << 20),
        name="attention",
    )(lengths, core, *inputs, *(far(w) for w in weights))


def swapped(blocks):
    size = blocks * blocks
    first = lax.broadcasted_iota(jnp.int32, (size, size), 0)
    second = lax.broadcasted_iota(jnp.int32, (size, size), 1)
    same = (first // blocks == second % blocks) & (first % blocks == second // blocks)
    return same.astype(F32).astype(BF16)


def stacked(values, first, blocks):
    rows = values[first : first + blocks]
    return jnp.concatenate([rows[:, j * LANES : (j + 1) * LANES] for j in range(blocks)], axis=0)


def dispatch_kernel(
    tokens_ref, own_ref, peer_ref, gain_ref, slots_any, send_ref, resid_ref, lines, slots, sem
):
    top, seqs = slots.shape
    copy = pltpu.make_async_copy(slots_any, slots, sem)
    copy.start()
    blocks = gain_ref.shape[0]
    mixed = own_ref[...].astype(F32) + peer_ref[...].astype(F32)
    resid = (tokens_ref[...].astype(F32) + mixed).astype(BF16)
    resid_ref[...] = resid
    expert_in = scaled_rows(resid.astype(F32), gain_ref[...].astype(F32))
    used = send_ref.shape[0]
    lines[...] = jnp.zeros(lines.shape, BF16)
    turn = swapped(blocks)
    by_token = [
        dot(turn, stacked(expert_in, first, blocks)).astype(BF16)
        for first in range(0, seqs, blocks)
    ]
    copy.wait()
    for t in range(seqs):
        start = t % blocks * blocks
        row = by_token[t // blocks][start : start + blocks]
        for k in range(top):
            slot = slots[k, t]
            place = jnp.where(slot < 0, used, slot * blocks)
            lines[pl.ds(pl.multiple_of(place, blocks), blocks), :] = row
    send_ref[...] = lines[:used]


def dispatch(used, tokens, own, peer, gain, slots):
    seqs, width = tokens.shape
    blocks = width // LANES
    vmem = pl.BlockSpec(memory_space=pltpu.VMEM)
    return pl.pallas_call(
        dispatch_kernel,
        out_shape=(pltpu.VMEM((used * blocks, LANES), BF16), pltpu.VMEM((seqs, width), BF16)),
        in_specs=[vmem] * 4 + [SLOTS_SPEC],
        out_specs=(vmem, vmem),
        scratch_shapes=[
            pltpu.VMEM(((used + 1) * blocks, LANES), BF16),
            pltpu.SMEM(slots.shape, jnp.int32),
            pltpu.SemaphoreType.DMA,
        ],
        compiler_params=pltpu.CompilerParams(vmem_limit_bytes=16 << 20),
        name="dispatch",
    )(near(tokens), near(own), near(peer), near(gain), near(slots))


def experts_kernel(
    lines_ref, gate_own, up_own, down_own, gate_peer, up_peer, down_peer, out_ref, rows
):
    count, width = rows.shape
    blocks = width // LANES
    size = blocks * blocks
    turn = swapped(blocks)
    for first in range(0, count, 2 * blocks):
        at = first * blocks
        both = [lines_ref[at : at + size], lines_ref[at + size : at + 2 * size]]
        turned = dot(turn, jnp.concatenate(both, axis=1)).astype(BF16)
        for i in range(2):
            start = first + i * blocks
            for j in range(blocks):
                rows[start : start + blocks, j * LANES : (j + 1) * LANES] = turned[
                    j * blocks : (j + 1) * blocks, i * LANES : (i + 1) * LANES
                ]

    def hidden(gate_w, up_w):
        gate = dot(rows[...], gate_w[...])
        return (gate / (1.0 + jnp.exp(-gate)) * dot(rows[...], up_w[...])).astype(BF16)

    act = jnp.concatenate([hidden(gate_own, up_own), hidden(gate_peer, up_peer)], axis=1)
    down = jnp.concatenate([down_own[...], down_peer[...]], axis=0)
    outputs = dot(act, down).astype(BF16)
    for first in range(0, count, 2 * blocks):
        both = [stacked(outputs, first + i * blocks, blocks) for i in range(2)]
        turned = dot(turn, jnp.concatenate(both, axis=1)).astype(BF16)
        for i in range(2):
            at = (first + i * blocks) * blocks
            out_ref[at : at + size] = turned[:, i * LANES : (i + 1) * LANES]


def experts(used, lines, *weights):
    vmem = pl.BlockSpec(memory_space=pltpu.VMEM)
    return pl.pallas_call(
        experts_kernel,
        out_shape=pltpu.VMEM(lines.shape, BF16),
        in_specs=[vmem] * 7,
        out_specs=vmem,
        scratch_shapes=[pltpu.VMEM((used, weights[0].shape[0]), BF16)],
        compiler_params=pltpu.CompilerParams(vmem_limit_bytes=32 << 20),
        name="experts",
    )(near(lines), *(near(w) for w in weights))


def combine_kernel(
    core, shares_any, slots_any, returned_ref, resid_ref, keep_ref, give_ref, wide, shares, slots, sems
):
    top, seqs = slots.shape
    copies = [
        pltpu.make_async_copy(slots_any, slots, sems.at[0]),
        pltpu.make_async_copy(shares_any, shares, sems.at[1]),
    ]
    for c in copies:
        c.start()
    for c in copies:
        c.wait()
    for t in range(seqs):
        total = jnp.zeros(wide.shape[1:], F32)
        for k in range(top):
            slot = slots[k, t]
            at = pl.multiple_of(jnp.maximum(slot, 0) * wide.shape[1], wide.shape[1])
            row = returned_ref[pl.ds(at, wide.shape[1]), :].astype(F32)
            total = total + jnp.where(slot >= 0, row * shares[k, t], 0.0)
        wide[t] = total
    half = wide.shape[1] // 2
    width = half * LANES
    mine = core[0]

    def columns(which):
        return jnp.concatenate([wide[:, which * half + j, :] for j in range(half)], axis=1)

    resid = jnp.where(mine == 0, resid_ref[:, :width], resid_ref[:, width:])
    keep_ref[...] = columns(mine) + resid.astype(F32)
    give_ref[...] = columns(1 - mine)


def combine(returned, slots, shares, resid, core):
    seqs, width = resid.shape
    blocks = width // LANES
    vmem = pl.BlockSpec(memory_space=pltpu.VMEM)
    half = pltpu.VMEM((seqs, width // 2), F32)
    return pl.pallas_call(
        combine_kernel,
        out_shape=(half, half),
        in_specs=[pl.BlockSpec(memory_space=pltpu.SMEM), SLOTS_SPEC, SLOTS_SPEC, vmem, vmem],
        out_specs=(vmem, vmem),
        scratch_shapes=[
            pltpu.VMEM((seqs, blocks, LANES), F32),
            pltpu.SMEM(shares.shape, F32),
            pltpu.SMEM(slots.shape, jnp.int32),
            pltpu.SemaphoreType.DMA((2,)),
        ],
        compiler_params=pltpu.CompilerParams(vmem_limit_bytes=16 << 20),
        name="combine",
    )(core, near(shares), near(slots), near(returned), near(resid))


SLOTS_SPEC = pl.BlockSpec(memory_space=pltpu.VMEM)


def near(array):
    return pltpu.with_memory_space_constraint(array, pltpu.VMEM)


def far(array):
    return pltpu.with_memory_space_constraint(array, pltpu.HBM)


def shards(
    tokens, norm_gain, expert_gain, w_query, key_weight, value_weight, forget_weight, w_out,
    key_cache, cached_values, cum_gates, lengths, routes, route_weights, expert_gate, expert_up,
    expert_down,
):
    seqs, width = tokens.shape
    head = key_cache.shape[3]
    n_exp = expert_gate.shape[0] * lax.axis_size("ep")
    share = max(2, 2 * seqs * routes.shape[1] // n_exp) // 2
    used, blocks = n_exp * share, width // LANES
    swap = [(0, 1), (1, 0)]
    core = lax.axis_index("tp").reshape(1)
    stored = (expert_gate[0], expert_up[0], expert_down[0])
    own, slots, *weights = attention(
        share, tokens, norm_gain.reshape(blocks, LANES), w_query, key_weight, value_weight,
        forget_weight.T, w_out, key_cache.reshape(-1, head),
        cached_values.reshape(-1, head), cum_gates.reshape(-1, LANES), lengths,
        routes.T, core, stored,
    )
    peer = lax.ppermute(own, "tp", swap)
    send, resid = dispatch(used, tokens, own, peer, expert_gain.reshape(blocks, LANES), slots)
    *weights, send = lax.optimization_barrier((*weights, send))
    other = tuple(lax.ppermute(w, "tp", swap) for w in weights)

    def exchange(lines):
        slabs = lines.reshape(n_exp, share * blocks, LANES)
        slabs = lax.all_to_all(slabs, "ep", split_axis=0, concat_axis=0, tiled=True)
        return slabs.reshape(used * blocks, LANES)

    outputs = experts(used, exchange(send), *weights, *other)
    keep, give = combine(exchange(outputs), slots, route_weights.T, resid, core)
    got = lax.ppermute(give, "tp", swap)
    return (keep + got).astype(BF16)


def solution(mesh):
    in_specs = (
        P("ep", None),
        P(),
        P(),
        P(None, "tp"),
        P(None, "tp"),
        P(None, "tp"),
        P(),
        P("tp", None),
        P("ep", None, "tp", None),
        P("ep", None, "tp", None),
        P("ep", "tp", None),
        P("ep"),
        P("ep", None),
        P("ep", None),
        P("ep", None, "tp"),
        P("ep", None, "tp"),
        P("ep", "tp", None),
    )
    out_specs = P("ep", "tp")
    return jax.shard_map(shards, mesh=mesh, in_specs=in_specs, out_specs=out_specs, check_vma=False)
```

```python
import functools
import jax
import jax.numpy as jnp
from jax import lax
from jax.experimental import pallas as pl
from jax.experimental.pallas import tpu as pltpu
from jax.sharding import PartitionSpec as P

EPS = 1e-06
LANES = 128
GROUP = 8
CHUNK = 256
SPANS = ((0,),(1,),(2,),(3,),(4,),(5,))
F32, BF16 = jnp.float32, jnp.bfloat16


def dot(a, b):
    return jnp.dot(a, b, preferred_element_type=F32)


def dot_nt(a, b):
    return lax.dot_general(a, b, (((1,), (1,)), ((), ())), preferred_element_type=F32)


def scaled_rows(flt, gain):
    scale = lax.rsqrt(jnp.mean(flt * flt, axis=-1, keepdims=True) + EPS)
    blocks = [
        flt[:, j * LANES : (j + 1) * LANES] * scale * gain[j : j + 1, :]
        for j in range(gain.shape[0])
    ]
    return jnp.concatenate(blocks, axis=1).astype(BF16)


def attention_kernel(
    share, n_exp, lengths, core, tokens_hbm, gain_hbm, wq_hbm, wk_hbm, wv_hbm, forget_hbm, wo_hbm,
    keys_hbm, values_hbm, gates_hbm, routes_hbm, gate_hbm, up_hbm, down_hbm, shares_hbm, partial_ref, places_ref,
    parts_ref, pack_ref,
    tokens, gain, wq, wk, wv, forget, wo, keys, values, gates, routes, attended,
    shares_ref, small_sems, key_sems, value_sems, weight_sems,
):
    seqs = attended.shape[0]
    places, head = keys.shape[0] // seqs, keys.shape[1]
    small = [
        (tokens_hbm, tokens), (gain_hbm, gain), (wq_hbm, wq), (wk_hbm, wk), (wv_hbm, wv),
        (forget_hbm, forget), (gates_hbm, gates), (routes_hbm, routes), (shares_hbm, shares_ref), (wo_hbm, wo),
    ]
    copies = [pltpu.make_async_copy(a, b, small_sems.at[i]) for i, (a, b) in enumerate(small)]

    def filled(s):
        return lax.shift_right_logical(lengths[s] + (LANES - 1), 7)

    def start(hbm, vmem, sems, which):
        for g in which:
            for s in range(g * GROUP, (g + 1) * GROUP):
                count = pl.multiple_of(lax.shift_left(filled(s), 7), LANES)
                at = pl.ds(s * places, count)
                pltpu.make_async_copy(hbm.at[at], vmem.at[at], sems.at[g]).start()

    def wait(hbm, vmem, sems, which):
        for g in which:
            count = sum(filled(s) for s in range(g * GROUP, (g + 1) * GROUP))
            at = pl.ds(0, pl.multiple_of(lax.shift_left(count, 7), LANES))
            pltpu.make_async_copy(hbm.at[at], vmem.at[at], sems.at[g]).wait()

    def start_values(which):
        for g in which:
            for s in range(g * GROUP, (g + 1) * GROUP):
                edge = jnp.minimum(filled(s), places // LANES - 1)
                at = pl.multiple_of(s * places + lax.shift_left(edge, 7), LANES)
                values[pl.ds(at, LANES), :] = jnp.zeros((LANES, head), BF16)
        start(values_hbm, values, value_sems, which)

    for c in copies[:-1]:
        c.start()
    spans = SPANS + ((), (), ())
    start(keys_hbm, keys, key_sems, spans[0])
    for c in copies[:2]:
        c.wait()
    normed = scaled_rows(tokens[...].astype(F32), gain[...].astype(F32))
    for c in copies[7:9]:
        c.wait()
    named = routes[...]
    top, blocks = named.shape[0], gain.shape[0]
    expert = lax.broadcasted_iota(jnp.int32, (n_exp, seqs), 0)
    hits = [expert == named[k : k + 1, :] for k in range(top)]
    onehot = sum(h.astype(F32) for h in hits)
    before = lax.broadcasted_iota(jnp.int32, (seqs, seqs), 0) < lax.broadcasted_iota(
        jnp.int32, (seqs, seqs), 1
    )
    count = dot(onehot.astype(BF16), before.astype(BF16))
    for k in range(top):
        rank = jnp.sum(jnp.where(hits[k], count, 0.0), axis=0, keepdims=True).astype(jnp.int32)
        rank = rank - core[0] * share
        mine = (rank >= 0) & (rank < share)
        place = (named[k : k + 1, :] * share + rank) * blocks
        places_ref[k : k + 1, :] = jnp.where(mine, place, n_exp * share * blocks)
        places_ref[top + k : top + k + 1, :] = jnp.where(mine, place, 0)
        parts_ref[k : k + 1, :] = jnp.where(mine, shares_ref[k : k + 1, :], 0.0)

    start(keys_hbm, keys, key_sems, spans[1])
    start_values(spans[0])
    for c in copies[2:6]:
        c.wait()
    query = dot(normed, wq[...]).astype(BF16)
    key_new = dot(normed, wk[...]).astype(BF16).astype(F32)
    value_new = dot(normed, wv[...]).astype(BF16).astype(F32)
    raw = dot_nt(normed, forget[...])
    column = lax.broadcasted_iota(jnp.int32, raw.shape, 1) == core[0]
    raw = jnp.sum(jnp.where(column, raw, 0.0), axis=1, keepdims=True)
    log_forget = jnp.minimum(raw, 0.0) - jnp.log1p(jnp.exp(-jnp.abs(raw)))

    start(keys_hbm, keys, key_sems, spans[2])
    start_values(spans[1])
    copies[-1].start()
    copies[6].wait()
    scale = head ** (-0.5)
    rows2 = lax.broadcasted_iota(jnp.int32, (2 * GROUP, 1), 0) % GROUP
    rows1 = lax.broadcasted_iota(jnp.int32, (GROUP, 1), 0)
    place = lax.broadcasted_iota(jnp.int32, (GROUP, places), 1)

    def scores_of(g):
        own_rows = slice(g * GROUP, (g + 1) * GROUP)
        q_two = jnp.concatenate([query[own_rows, :head], query[own_rows, head:]], axis=0)
        raw_scores = jnp.zeros((2 * GROUP, places), F32)
        for i in range(GROUP):
            raw_scores = jnp.where(
                rows2 == i, dot_nt(q_two, keys[(g * GROUP + i) * places : (g * GROUP + i + 1) * places]), raw_scores
            )
        return q_two, raw_scores

    def probs_of(g, q_two, raw_scores):
        own_rows = slice(g * GROUP, (g + 1) * GROUP)
        size = jnp.zeros((GROUP, 1), jnp.int32)
        for i in range(GROUP):
            size = jnp.where(rows1 == i, lengths[g * GROUP + i], size)
        steps = places // LANES
        cum = jnp.concatenate(
            [gates[pl.ds(g * GROUP * steps + j, GROUP, stride=steps), :] for j in range(steps)],
            axis=1,
        )
        last = jnp.sum(jnp.where(place == size - 1, cum, 0.0), axis=1, keepdims=True)
        bias = (log_forget[own_rows] + last) - cum
        valid = place < size
        both = jnp.concatenate([bias, bias], axis=0)
        keep = jnp.concatenate([size, size], axis=0)
        scores = raw_scores * scale + both
        place2 = lax.broadcasted_iota(jnp.int32, (2 * GROUP, places), 1)
        scores = jnp.where(place2 < keep, scores, -jnp.inf)
        k_two = jnp.concatenate([key_new[own_rows], key_new[own_rows]], axis=0)
        own = jnp.sum(q_two.astype(F32) * k_two, axis=1, keepdims=True) * scale
        peak = jnp.maximum(jnp.max(scores, axis=1, keepdims=True), own)
        expo = jnp.exp(scores - peak)
        own_expo = jnp.exp(own - peak)
        denom = jnp.sum(expo, axis=1, keepdims=True) + own_expo
        inverse = 1.0 / denom
        probs = (expo * inverse).astype(BF16)
        own_prob = (own_expo * inverse).astype(BF16).astype(F32)
        v_two = jnp.concatenate([value_new[own_rows], value_new[own_rows]], axis=0)
        return probs, own_prob * v_two

    def result_of(g, probs, own):
        result = own
        for i in range(GROUP):
            s = g * GROUP + i
            for c in range(0, places, CHUNK):
                part = dot(probs[:, c : c + CHUNK], values[s * places + c : s * places + c + CHUNK])
                used = rows2 == i
                if c:
                    used = used & (lengths[s] > c)
                result = result + jnp.where(used, part, 0.0)
        result = result.astype(BF16)
        own_rows = slice(g * GROUP, (g + 1) * GROUP)
        attended[own_rows, :head] = result[:GROUP]
        attended[own_rows, head:] = result[GROUP:]

    wait(keys_hbm, keys, key_sems, spans[0])
    width, inner = gate_hbm.shape
    pairs = [(gate_hbm, pack_ref.at[:width]), (up_hbm, pack_ref.at[width : 2 * width])]
    for first in range(0, width, inner):
        at = 2 * width + first
        pairs.append((down_hbm.at[:, first : first + inner], pack_ref.at[at : at + inner]))
    moved = [pltpu.make_async_copy(a, b, weight_sems.at[i]) for i, (a, b) in enumerate(pairs)]
    pending = [scores_of(g) for g in spans[0]]
    for i, span in enumerate(SPANS):
        start(keys_hbm, keys, key_sems, spans[i + 3])
        start_values(spans[i + 2])
        if i + 3 == len(SPANS):
            for c in moved:
                c.start()
        wait(values_hbm, values, value_sems, span)
        wait(keys_hbm, keys, key_sems, spans[i + 1])
        ready = [probs_of(g, *p) for g, p in zip(span, pending)]
        pending = [scores_of(g) for g in spans[i + 1]]
        for g, (probs, own) in zip(span, ready):
            result_of(g, probs, own)
    for c in moved:
        c.wait()
    copies[-1].wait()
    partial_ref[...] = dot(attended[...], wo[...]).astype(BF16)


def attention(
    share, n_exp, tokens, gain, wq, wk, wv, forget, wo, keys, values, gates, lengths, routes, core,
    weights, shares,
):
    seqs = tokens.shape[0]
    anywhere = pl.BlockSpec(memory_space=pl.ANY)
    hbm = pl.BlockSpec(memory_space=pltpu.HBM)
    scalar = pl.BlockSpec(memory_space=pltpu.SMEM)
    inputs = (tokens, gain, wq, wk, wv, forget, wo, keys, values, gates, routes)
    order = (tokens, gain, wq, wk, wv, forget, wo, keys, values, gates, routes)
    return pl.pallas_call(
        functools.partial(attention_kernel, share, n_exp),
        out_shape=(
            pltpu.VMEM(tokens.shape, BF16),
            pltpu.VMEM((2 * routes.shape[0], routes.shape[1]), jnp.int32),
            pltpu.VMEM(routes.shape, F32),
            pltpu.VMEM((3 * weights[0].shape[0], weights[0].shape[1]), BF16),
        ),
        in_specs=[scalar, scalar] + [anywhere] * len(inputs)
        + [hbm] * len(weights)
        + [anywhere],
        out_specs=[pl.BlockSpec(memory_space=pltpu.VMEM)] * 4,
        scratch_shapes=[pltpu.VMEM(a.shape, a.dtype) for a in order]
        + [
            pltpu.VMEM((seqs, wo.shape[0]), BF16),
            pltpu.VMEM(shares.shape, F32),
            pltpu.SemaphoreType.DMA((10,)),
            pltpu.SemaphoreType.DMA((seqs // GROUP,)),
            pltpu.SemaphoreType.DMA((seqs // GROUP,)),
            pltpu.SemaphoreType.DMA((2 + weights[0].shape[0] // weights[0].shape[1],)),
        ],
        compiler_params=pltpu.CompilerParams(vmem_limit_bytes=52 << 20),
        name="attention",
    )(lengths, core, *inputs, *(far(w) for w in weights), shares)


def swapped(blocks):
    size = blocks * blocks
    first = lax.broadcasted_iota(jnp.int32, (size, size), 0)
    second = lax.broadcasted_iota(jnp.int32, (size, size), 1)
    same = (first // blocks == second % blocks) & (first % blocks == second // blocks)
    return same.astype(F32).astype(BF16)


def stacked(values, first, blocks):
    rows = values[first : first + blocks]
    return jnp.concatenate([rows[:, j * LANES : (j + 1) * LANES] for j in range(blocks)], axis=0)


def dispatch_kernel(
    tokens_ref, own_ref, peer_ref, gain_ref, slots_any, send_ref, resid_ref, lines, slots, sem
):
    top, seqs = slots.shape[0] // 2, slots.shape[1]
    copy = pltpu.make_async_copy(slots_any, slots, sem)
    copy.start()
    blocks = gain_ref.shape[0]
    mixed = own_ref[...].astype(F32) + peer_ref[...].astype(F32)
    resid = (tokens_ref[...].astype(F32) + mixed).astype(BF16)
    resid_ref[...] = resid
    expert_in = scaled_rows(resid.astype(F32), gain_ref[...].astype(F32))
    used = send_ref.shape[0]
    lines[...] = jnp.zeros(lines.shape, BF16)
    turn = swapped(blocks)
    by_token = [
        dot(turn, stacked(expert_in, first, blocks)).astype(BF16)
        for first in range(0, seqs, blocks)
    ]
    copy.wait()
    for t in range(seqs):
        start = t % blocks * blocks
        row = by_token[t // blocks][start : start + blocks]
        for k in range(top):
            lines[pl.ds(pl.multiple_of(slots[k, t], blocks), blocks), :] = row
    send_ref[...] = lines[:used]


def dispatch(used, tokens, own, peer, gain, slots):
    seqs, width = tokens.shape
    blocks = width // LANES
    vmem = pl.BlockSpec(memory_space=pltpu.VMEM)
    return pl.pallas_call(
        dispatch_kernel,
        out_shape=(pltpu.VMEM((used * blocks, LANES), BF16), pltpu.VMEM((seqs, width), BF16)),
        in_specs=[vmem] * 4 + [SLOTS_SPEC],
        out_specs=(vmem, vmem),
        scratch_shapes=[
            pltpu.VMEM(((used + 1) * blocks, LANES), BF16),
            pltpu.SMEM(slots.shape, jnp.int32),
            pltpu.SemaphoreType.DMA,
        ],
        compiler_params=pltpu.CompilerParams(vmem_limit_bytes=16 << 20),
        name="dispatch",
    )(near(tokens), near(own), near(peer), near(gain), near(slots))


def experts_kernel(lines_ref, own_ref, peer_ref, out_ref, rows):
    count, width = rows.shape
    blocks = width // LANES
    size = blocks * blocks
    turn = swapped(blocks)
    for first in range(0, count, 2 * blocks):
        at = first * blocks
        both = [lines_ref[at : at + size], lines_ref[at + size : at + 2 * size]]
        turned = dot(turn, jnp.concatenate(both, axis=1)).astype(BF16)
        for i in range(2):
            start = first + i * blocks
            for j in range(blocks):
                rows[start : start + blocks, j * LANES : (j + 1) * LANES] = turned[
                    j * blocks : (j + 1) * blocks, i * LANES : (i + 1) * LANES
                ]

    inner = own_ref.shape[1]

    def hidden(pack):
        gate = dot(rows[...], pack[:width])
        upper = dot(rows[...], pack[width : 2 * width])
        return (gate / (1.0 + jnp.exp(-gate)) * upper).astype(BF16)

    act = jnp.concatenate([hidden(own_ref), hidden(peer_ref)], axis=1)
    outputs = []
    for first in range(2 * width, 3 * width, inner):
        down = [pack[first : first + inner] for pack in (own_ref, peer_ref)]
        outputs.append(dot(act, jnp.concatenate(down, axis=0)).astype(BF16))
    outputs = jnp.concatenate(outputs, axis=1)
    for first in range(0, count, 2 * blocks):
        both = [stacked(outputs, first + i * blocks, blocks) for i in range(2)]
        turned = dot(turn, jnp.concatenate(both, axis=1)).astype(BF16)
        for i in range(2):
            at = (first + i * blocks) * blocks
            out_ref[at : at + size] = turned[:, i * LANES : (i + 1) * LANES]


def experts(used, lines, own, peer):
    vmem = pl.BlockSpec(memory_space=pltpu.VMEM)
    return pl.pallas_call(
        experts_kernel,
        out_shape=pltpu.VMEM(lines.shape, BF16),
        in_specs=[vmem] * 3,
        out_specs=vmem,
        scratch_shapes=[pltpu.VMEM((used, own.shape[0] // 3), BF16)],
        compiler_params=pltpu.CompilerParams(vmem_limit_bytes=32 << 20),
        name="experts",
    )(near(lines), near(own), near(peer))


def combine_kernel(
    kept, core, shares_any, slots_any, returned_ref, *refs
):
    *resid_refs, out_ref, wide, shares, slots, sems = refs
    top, seqs = shares.shape
    copies = [
        pltpu.make_async_copy(slots_any, slots, sems.at[0]),
        pltpu.make_async_copy(shares_any, shares, sems.at[1]),
    ]
    for c in copies:
        c.start()
    half = wide.shape[1]
    which = core[0] if kept else 1 - core[0]
    first = which * half
    for c in copies:
        c.wait()
    for t in range(seqs):
        total = jnp.zeros(wide.shape[1:], F32)
        for k in range(top):
            at = pl.multiple_of(slots[top + k, t] + first, half)
            total = total + returned_ref[pl.ds(at, half), :].astype(F32) * shares[k, t]
        wide[t] = total
    columns = jnp.concatenate([wide[:, j, :] for j in range(half)], axis=1)
    for ref in resid_refs:
        width = half * LANES
        resid = jnp.where(which == 0, ref[:, :width], ref[:, width:])
        columns = columns + resid.astype(F32)
    out_ref[...] = columns


def combine(half, kept, returned, slots, shares, core, *resid):
    seqs = slots.shape[1]
    vmem = pl.BlockSpec(memory_space=pltpu.VMEM)
    return pl.pallas_call(
        functools.partial(combine_kernel, kept),
        out_shape=pltpu.VMEM((seqs, half * LANES), F32),
        in_specs=[pl.BlockSpec(memory_space=pltpu.SMEM)] + [vmem] * (3 + len(resid)),
        out_specs=vmem,
        scratch_shapes=[
            pltpu.VMEM((seqs, half, LANES), F32),
            pltpu.SMEM(shares.shape, F32),
            pltpu.SMEM(slots.shape, jnp.int32),
            pltpu.SemaphoreType.DMA((2,)),
        ],
        compiler_params=pltpu.CompilerParams(vmem_limit_bytes=16 << 20),
        name="keep" if kept else "give",
    )(core, near(shares), near(slots), near(returned), *(near(r) for r in resid))


SLOTS_SPEC = pl.BlockSpec(memory_space=pltpu.VMEM)


def near(array):
    return pltpu.with_memory_space_constraint(array, pltpu.VMEM)


def far(array):
    return pltpu.with_memory_space_constraint(array, pltpu.HBM)


def shards(
    tokens, norm_gain, expert_gain, w_query, key_weight, value_weight, forget_weight, w_out,
    key_cache, cached_values, cum_gates, lengths, routes, route_weights, expert_gate, expert_up,
    expert_down,
):
    seqs, width = tokens.shape
    head = key_cache.shape[3]
    n_exp = expert_gate.shape[0] * lax.axis_size("ep")
    share = max(2, 2 * seqs * routes.shape[1] // n_exp) // 2
    used, blocks = n_exp * share, width // LANES
    swap = [(0, 1), (1, 0)]
    core = lax.axis_index("tp").reshape(1)
    stored = (expert_gate[0], expert_up[0], expert_down[0])
    own, slots, parts, pack = attention(
        share, n_exp, tokens, norm_gain.reshape(blocks, LANES), w_query, key_weight, value_weight,
        forget_weight.T, w_out, key_cache.reshape(-1, head),
        cached_values.reshape(-1, head), cum_gates.reshape(-1, LANES), lengths,
        routes.T, core, stored, route_weights.T,
    )
    peer = lax.ppermute(own, "tp", swap)
    send, resid = dispatch(used, tokens, own, peer, expert_gain.reshape(blocks, LANES), slots)
    pack, send = lax.optimization_barrier((pack, send))
    other = lax.ppermute(pack, "tp", swap)

    def exchange(lines):
        slabs = lines.reshape(n_exp, share * blocks, LANES)
        slabs = lax.all_to_all(slabs, "ep", split_axis=0, concat_axis=0, tiled=True)
        return slabs.reshape(used * blocks, LANES)

    outputs = experts(used, exchange(send), pack, other)
    returned = exchange(outputs)
    give = combine(blocks // 2, False, returned, slots, parts, core)
    got = lax.ppermute(give, "tp", swap)
    keep = combine(blocks // 2, True, returned, slots, parts, core, resid)
    return (keep + got).astype(BF16)


def solution(mesh):
    in_specs = (
        P("ep", None),
        P(),
        P(),
        P(None, "tp"),
        P(None, "tp"),
        P(None, "tp"),
        P(),
        P("tp", None),
        P("ep", None, "tp", None),
        P("ep", None, "tp", None),
        P("ep", "tp", None),
        P("ep"),
        P("ep", None),
        P("ep", None),
        P("ep", None, "tp"),
        P("ep", None, "tp"),
        P("ep", "tp", None),
    )
    out_specs = P("ep", "tp")
    return jax.shard_map(shards, mesh=mesh, in_specs=in_specs, out_specs=out_specs, check_vma=False)
```

```python
import functools
import jax
import jax.numpy as jnp
from jax import lax
from jax.experimental import pallas as pl
from jax.experimental.pallas import tpu as pltpu
from jax.sharding import PartitionSpec as P

EPS = 1e-06
LANES = 128
GROUP = 8
CHUNK = 256
SPANS = ((0,),(1,),(2,),(3,),(4,),(5,))
F32, BF16 = jnp.float32, jnp.bfloat16


def dot(a, b):
    return jnp.dot(a, b, preferred_element_type=F32)


def dot_nt(a, b):
    return lax.dot_general(a, b, (((1,), (1,)), ((), ())), preferred_element_type=F32)


def scaled_rows(flt, gain):
    scale = lax.rsqrt(jnp.mean(flt * flt, axis=-1, keepdims=True) + EPS)
    blocks = [
        flt[:, j * LANES : (j + 1) * LANES] * scale * gain[j : j + 1, :]
        for j in range(gain.shape[0])
    ]
    return jnp.concatenate(blocks, axis=1).astype(BF16)


def attention_kernel(
    share, n_exp, lengths, core, tokens_hbm, gain_hbm, wq_hbm, wk_hbm, wv_hbm, forget_hbm, wo_hbm,
    keys_hbm, values_hbm, gates_hbm, routes_hbm, gate_hbm, up_hbm, down_hbm, shares_hbm, partial_ref, places_ref,
    parts_ref, pack_ref,
    tokens, gain, wq, wk, wv, forget, wo, keys, values, gates, routes, attended,
    shares_ref, small_sems, key_sems, value_sems, weight_sems,
):
    seqs = attended.shape[0]
    places, head = keys.shape[0] // seqs, keys.shape[1]
    small = [
        (tokens_hbm, tokens), (gain_hbm, gain), (wq_hbm, wq), (wk_hbm, wk), (wv_hbm, wv),
        (forget_hbm, forget), (gates_hbm, gates), (routes_hbm, routes), (shares_hbm, shares_ref), (wo_hbm, wo),
    ]
    copies = [pltpu.make_async_copy(a, b, small_sems.at[i]) for i, (a, b) in enumerate(small)]

    def filled(s):
        return lax.shift_right_logical(lengths[s] + (LANES - 1), 7)

    def start(hbm, vmem, sems, which):
        for g in which:
            for s in range(g * GROUP, (g + 1) * GROUP):
                count = pl.multiple_of(lax.shift_left(filled(s), 7), LANES)
                at = pl.ds(s * places, count)
                pltpu.make_async_copy(hbm.at[at], vmem.at[at], sems.at[g]).start()

    def wait(hbm, vmem, sems, which):
        for g in which:
            count = sum(filled(s) for s in range(g * GROUP, (g + 1) * GROUP))
            at = pl.ds(0, pl.multiple_of(lax.shift_left(count, 7), LANES))
            pltpu.make_async_copy(hbm.at[at], vmem.at[at], sems.at[g]).wait()

    def start_values(which):
        for g in which:
            for s in range(g * GROUP, (g + 1) * GROUP):
                edge = jnp.minimum(filled(s), places // LANES - 1)
                at = pl.multiple_of(s * places + lax.shift_left(edge, 7), LANES)
                values[pl.ds(at, LANES), :] = jnp.zeros((LANES, head), BF16)
        start(values_hbm, values, value_sems, which)

    for c in copies[:-1]:
        c.start()
    spans = SPANS + ((), (), ())
    start(keys_hbm, keys, key_sems, spans[0])
    for c in copies[:2]:
        c.wait()
    normed = scaled_rows(tokens[...].astype(F32), gain[...].astype(F32))
    for c in copies[7:9]:
        c.wait()
    named = routes[...]
    top, blocks = named.shape[0], gain.shape[0]
    expert = lax.broadcasted_iota(jnp.int32, (n_exp, seqs), 0)
    hits = [expert == named[k : k + 1, :] for k in range(top)]
    onehot = sum(h.astype(F32) for h in hits)
    before = lax.broadcasted_iota(jnp.int32, (seqs, seqs), 0) < lax.broadcasted_iota(
        jnp.int32, (seqs, seqs), 1
    )
    count = dot(onehot.astype(BF16), before.astype(BF16))
    for k in range(top):
        rank = jnp.sum(jnp.where(hits[k], count, 0.0), axis=0, keepdims=True).astype(jnp.int32)
        rank = rank - core[0] * share
        mine = (rank >= 0) & (rank < share)
        place = (named[k : k + 1, :] * share + rank) * blocks
        places_ref[k : k + 1, :] = jnp.where(mine, place, n_exp * share * blocks)
        places_ref[top + k : top + k + 1, :] = jnp.where(mine, place, 0)
        parts_ref[k : k + 1, :] = jnp.where(mine, shares_ref[k : k + 1, :], 0.0)

    start(keys_hbm, keys, key_sems, spans[1])
    start_values(spans[0])
    for c in copies[2:6]:
        c.wait()
    query = dot(normed, wq[...]).astype(BF16)
    key_new = dot(normed, wk[...]).astype(BF16).astype(F32)
    value_new = dot(normed, wv[...]).astype(BF16).astype(F32)
    raw = dot_nt(normed, forget[...])
    column = lax.broadcasted_iota(jnp.int32, raw.shape, 1) == core[0]
    raw = jnp.sum(jnp.where(column, raw, 0.0), axis=1, keepdims=True)
    log_forget = jnp.minimum(raw, 0.0) - jnp.log1p(jnp.exp(-jnp.abs(raw)))

    start(keys_hbm, keys, key_sems, spans[2])
    start_values(spans[1])
    copies[-1].start()
    copies[6].wait()
    scale = head ** (-0.5)
    rows2 = lax.broadcasted_iota(jnp.int32, (2 * GROUP, 1), 0) % GROUP
    rows1 = lax.broadcasted_iota(jnp.int32, (GROUP, 1), 0)
    place = lax.broadcasted_iota(jnp.int32, (GROUP, places), 1)

    def scores_of(g):
        own_rows = slice(g * GROUP, (g + 1) * GROUP)
        q_two = jnp.concatenate([query[own_rows, :head], query[own_rows, head:]], axis=0)
        raw_scores = jnp.zeros((2 * GROUP, places), F32)
        for i in range(GROUP):
            raw_scores = jnp.where(
                rows2 == i, dot_nt(q_two, keys[(g * GROUP + i) * places : (g * GROUP + i + 1) * places]), raw_scores
            )
        return q_two, raw_scores

    def probs_of(g, q_two, raw_scores):
        own_rows = slice(g * GROUP, (g + 1) * GROUP)
        size = jnp.zeros((GROUP, 1), jnp.int32)
        for i in range(GROUP):
            size = jnp.where(rows1 == i, lengths[g * GROUP + i], size)
        steps = places // LANES
        cum = jnp.concatenate(
            [gates[pl.ds(g * GROUP * steps + j, GROUP, stride=steps), :] for j in range(steps)],
            axis=1,
        )
        last = jnp.sum(jnp.where(place == size - 1, cum, 0.0), axis=1, keepdims=True)
        bias = (log_forget[own_rows] + last) - cum
        valid = place < size
        both = jnp.concatenate([bias, bias], axis=0)
        keep = jnp.concatenate([size, size], axis=0)
        scores = raw_scores * scale + both
        place2 = lax.broadcasted_iota(jnp.int32, (2 * GROUP, places), 1)
        scores = jnp.where(place2 < keep, scores, -jnp.inf)
        k_two = jnp.concatenate([key_new[own_rows], key_new[own_rows]], axis=0)
        own = jnp.sum(q_two.astype(F32) * k_two, axis=1, keepdims=True) * scale
        peak = jnp.maximum(jnp.max(scores, axis=1, keepdims=True), own)
        expo = jnp.exp(scores - peak)
        own_expo = jnp.exp(own - peak)
        denom = jnp.sum(expo, axis=1, keepdims=True) + own_expo
        inverse = 1.0 / denom
        probs = (expo * inverse).astype(BF16)
        own_prob = (own_expo * inverse).astype(BF16).astype(F32)
        v_two = jnp.concatenate([value_new[own_rows], value_new[own_rows]], axis=0)
        return probs, own_prob * v_two

    def result_of(g, probs, own):
        result = own
        for i in range(GROUP):
            s = g * GROUP + i
            for c in range(0, places, CHUNK):
                part = dot(probs[:, c : c + CHUNK], values[s * places + c : s * places + c + CHUNK])
                used = rows2 == i
                if c:
                    used = used & (lengths[s] > c)
                result = result + jnp.where(used, part, 0.0)
        result = result.astype(BF16)
        own_rows = slice(g * GROUP, (g + 1) * GROUP)
        attended[own_rows, :head] = result[:GROUP]
        attended[own_rows, head:] = result[GROUP:]

    wait(keys_hbm, keys, key_sems, spans[0])
    width, inner = gate_hbm.shape
    pairs = [(gate_hbm, pack_ref.at[:width]), (up_hbm, pack_ref.at[width : 2 * width])]
    for first in range(0, width, inner):
        at = 2 * width + first
        pairs.append((down_hbm.at[:, first : first + inner], pack_ref.at[at : at + inner]))
    moved = [pltpu.make_async_copy(a, b, weight_sems.at[i]) for i, (a, b) in enumerate(pairs)]
    pending = [scores_of(g) for g in spans[0]]
    for i, span in enumerate(SPANS):
        start(keys_hbm, keys, key_sems, spans[i + 3])
        start_values(spans[i + 2])
        if i + 3 == len(SPANS):
            for c in moved:
                c.start()
        wait(values_hbm, values, value_sems, span)
        wait(keys_hbm, keys, key_sems, spans[i + 1])
        ready = [probs_of(g, *p) for g, p in zip(span, pending)]
        pending = [scores_of(g) for g in spans[i + 1]]
        for g, (probs, own) in zip(span, ready):
            result_of(g, probs, own)
    for c in moved:
        c.wait()
    copies[-1].wait()
    partial_ref[...] = dot(attended[...], wo[...]).astype(BF16)


def attention(
    share, n_exp, tokens, gain, wq, wk, wv, forget, wo, keys, values, gates, lengths, routes, core,
    weights, shares,
):
    seqs = tokens.shape[0]
    anywhere = pl.BlockSpec(memory_space=pl.ANY)
    hbm = pl.BlockSpec(memory_space=pltpu.HBM)
    scalar = pl.BlockSpec(memory_space=pltpu.SMEM)
    inputs = (tokens, gain, wq, wk, wv, forget, wo, keys, values, gates, routes)
    order = (tokens, gain, wq, wk, wv, forget, wo, keys, values, gates, routes)
    return pl.pallas_call(
        functools.partial(attention_kernel, share, n_exp),
        out_shape=(
            pltpu.VMEM(tokens.shape, BF16),
            pltpu.VMEM((2 * routes.shape[0], routes.shape[1]), jnp.int32),
            pltpu.VMEM(routes.shape, F32),
            pltpu.VMEM((3 * weights[0].shape[0], weights[0].shape[1]), BF16),
        ),
        in_specs=[scalar, scalar] + [anywhere] * len(inputs)
        + [hbm] * len(weights)
        + [anywhere],
        out_specs=[pl.BlockSpec(memory_space=pltpu.VMEM)] * 4,
        scratch_shapes=[pltpu.VMEM(a.shape, a.dtype) for a in order]
        + [
            pltpu.VMEM((seqs, wo.shape[0]), BF16),
            pltpu.VMEM(shares.shape, F32),
            pltpu.SemaphoreType.DMA((10,)),
            pltpu.SemaphoreType.DMA((seqs // GROUP,)),
            pltpu.SemaphoreType.DMA((seqs // GROUP,)),
            pltpu.SemaphoreType.DMA((2 + weights[0].shape[0] // weights[0].shape[1],)),
        ],
        compiler_params=pltpu.CompilerParams(vmem_limit_bytes=52 << 20),
        name="attention",
    )(lengths, core, *inputs, *(far(w) for w in weights), shares)


def swapped(blocks):
    size = blocks * blocks
    first = lax.broadcasted_iota(jnp.int32, (size, size), 0)
    second = lax.broadcasted_iota(jnp.int32, (size, size), 1)
    same = (first // blocks == second % blocks) & (first % blocks == second // blocks)
    return same.astype(F32).astype(BF16)


def stacked(values, first, blocks):
    rows = values[first : first + blocks]
    return jnp.concatenate([rows[:, j * LANES : (j + 1) * LANES] for j in range(blocks)], axis=0)


def dispatch_kernel(
    tokens_ref, own_ref, peer_ref, gain_ref, slots_any, send_ref, resid_ref, lines, slots, sem
):
    top, seqs = slots.shape[0] // 2, slots.shape[1]
    copy = pltpu.make_async_copy(slots_any, slots, sem)
    copy.start()
    blocks = gain_ref.shape[0]
    mixed = own_ref[...].astype(F32) + peer_ref[...].astype(F32)
    resid = (tokens_ref[...].astype(F32) + mixed).astype(BF16)
    resid_ref[...] = resid
    expert_in = scaled_rows(resid.astype(F32), gain_ref[...].astype(F32))
    used = send_ref.shape[0]
    lines[...] = jnp.zeros(lines.shape, BF16)
    turn = swapped(blocks)
    by_token = [
        dot(turn, stacked(expert_in, first, blocks)).astype(BF16)
        for first in range(0, seqs, blocks)
    ]
    copy.wait()
    for t in range(seqs):
        start = t % blocks * blocks
        row = by_token[t // blocks][start : start + blocks]
        for k in range(top):
            lines[pl.ds(pl.multiple_of(slots[k, t], blocks), blocks), :] = row
    send_ref[...] = lines[:used]


def dispatch(used, tokens, own, peer, gain, slots):
    seqs, width = tokens.shape
    blocks = width // LANES
    vmem = pl.BlockSpec(memory_space=pltpu.VMEM)
    return pl.pallas_call(
        dispatch_kernel,
        out_shape=(pltpu.VMEM((used * blocks, LANES), BF16), pltpu.VMEM((seqs, width), BF16)),
        in_specs=[vmem] * 4 + [SLOTS_SPEC],
        out_specs=(vmem, vmem),
        scratch_shapes=[
            pltpu.VMEM(((used + 1) * blocks, LANES), BF16),
            pltpu.SMEM(slots.shape, jnp.int32),
            pltpu.SemaphoreType.DMA,
        ],
        compiler_params=pltpu.CompilerParams(vmem_limit_bytes=16 << 20),
        name="dispatch",
    )(near(tokens), near(own), near(peer), near(gain), near(slots))


def experts_kernel(lines_ref, own_ref, peer_ref, out_ref, rows):
    count, width = rows.shape
    blocks = width // LANES
    size = blocks * blocks
    turn = swapped(blocks)
    for first in range(0, count, 2 * blocks):
        at = first * blocks
        both = [lines_ref[at : at + size], lines_ref[at + size : at + 2 * size]]
        turned = dot(turn, jnp.concatenate(both, axis=1)).astype(BF16)
        for i in range(2):
            start = first + i * blocks
            for j in range(blocks):
                rows[start : start + blocks, j * LANES : (j + 1) * LANES] = turned[
                    j * blocks : (j + 1) * blocks, i * LANES : (i + 1) * LANES
                ]

    inner = own_ref.shape[1]

    def hidden(pack):
        gate = dot(rows[...], pack[:width])
        upper = dot(rows[...], pack[width : 2 * width])
        return (gate / (1.0 + jnp.exp(-gate)) * upper).astype(BF16)

    act = jnp.concatenate([hidden(own_ref), hidden(peer_ref)], axis=1)
    outputs = []
    for first in range(2 * width, 3 * width, inner):
        down = [pack[first : first + inner] for pack in (own_ref, peer_ref)]
        outputs.append(dot(act, jnp.concatenate(down, axis=0)).astype(BF16))
    outputs = jnp.concatenate(outputs, axis=1)
    for first in range(0, count, 2 * blocks):
        both = [stacked(outputs, first + i * blocks, blocks) for i in range(2)]
        turned = dot(turn, jnp.concatenate(both, axis=1)).astype(BF16)
        for i in range(2):
            at = (first + i * blocks) * blocks
            out_ref[at : at + size] = turned[:, i * LANES : (i + 1) * LANES]


def experts(used, lines, own, peer):
    vmem = pl.BlockSpec(memory_space=pltpu.VMEM)
    return pl.pallas_call(
        experts_kernel,
        out_shape=pltpu.VMEM(lines.shape, BF16),
        in_specs=[vmem] * 3,
        out_specs=vmem,
        scratch_shapes=[pltpu.VMEM((used, own.shape[0] // 3), BF16)],
        compiler_params=pltpu.CompilerParams(vmem_limit_bytes=32 << 20),
        name="experts",
    )(near(lines), near(own), near(peer))


def combine_kernel(
    kept, core, shares_any, slots_any, returned_ref, *refs
):
    *resid_refs, out_ref, wide, shares, slots, sems = refs
    top, seqs = shares.shape
    copies = [
        pltpu.make_async_copy(slots_any, slots, sems.at[0]),
        pltpu.make_async_copy(shares_any, shares, sems.at[1]),
    ]
    for c in copies:
        c.start()
    half = wide.shape[1]
    which = core[0] if kept else 1 - core[0]
    first = which * half
    for c in copies:
        c.wait()
    for t in range(seqs):
        total = jnp.zeros(wide.shape[1:], F32)
        for k in range(top):
            at = pl.multiple_of(slots[top + k, t] + first, half)
            total = total + returned_ref[pl.ds(at, half), :].astype(F32) * shares[k, t]
        wide[t] = total
    columns = jnp.concatenate([wide[:, j, :] for j in range(half)], axis=1)
    for ref in resid_refs:
        width = half * LANES
        resid = jnp.where(which == 0, ref[:, :width], ref[:, width:])
        columns = columns + resid.astype(F32)
    out_ref[...] = columns.astype(out_ref.dtype)


def combine(half, kept, returned, slots, shares, core, *resid):
    seqs = slots.shape[1]
    vmem = pl.BlockSpec(memory_space=pltpu.VMEM)
    return pl.pallas_call(
        functools.partial(combine_kernel, kept),
        out_shape=pltpu.VMEM((seqs, half * LANES), F32 if kept else BF16),
        in_specs=[pl.BlockSpec(memory_space=pltpu.SMEM)] + [vmem] * (3 + len(resid)),
        out_specs=vmem,
        scratch_shapes=[
            pltpu.VMEM((seqs, half, LANES), F32),
            pltpu.SMEM(shares.shape, F32),
            pltpu.SMEM(slots.shape, jnp.int32),
            pltpu.SemaphoreType.DMA((2,)),
        ],
        compiler_params=pltpu.CompilerParams(vmem_limit_bytes=16 << 20),
        name="keep" if kept else "give",
    )(core, near(shares), near(slots), near(returned), *(near(r) for r in resid))


SLOTS_SPEC = pl.BlockSpec(memory_space=pltpu.VMEM)


def near(array):
    return pltpu.with_memory_space_constraint(array, pltpu.VMEM)


def far(array):
    return pltpu.with_memory_space_constraint(array, pltpu.HBM)


def shards(
    tokens, norm_gain, expert_gain, w_query, key_weight, value_weight, forget_weight, w_out,
    key_cache, cached_values, cum_gates, lengths, routes, route_weights, expert_gate, expert_up,
    expert_down,
):
    seqs, width = tokens.shape
    head = key_cache.shape[3]
    n_exp = expert_gate.shape[0] * lax.axis_size("ep")
    share = max(2, 2 * seqs * routes.shape[1] // n_exp) // 2
    used, blocks = n_exp * share, width // LANES
    swap = [(0, 1), (1, 0)]
    core = lax.axis_index("tp").reshape(1)
    stored = (expert_gate[0], expert_up[0], expert_down[0])
    own, slots, parts, pack = attention(
        share, n_exp, tokens, norm_gain.reshape(blocks, LANES), w_query, key_weight, value_weight,
        forget_weight.T, w_out, key_cache.reshape(-1, head),
        cached_values.reshape(-1, head), cum_gates.reshape(-1, LANES), lengths,
        routes.T, core, stored, route_weights.T,
    )
    peer = lax.ppermute(own, "tp", swap)
    send, resid = dispatch(used, tokens, own, peer, expert_gain.reshape(blocks, LANES), slots)
    pack, send = lax.optimization_barrier((pack, send))
    other = lax.ppermute(pack, "tp", swap)

    def exchange(lines):
        slabs = lines.reshape(n_exp, share * blocks, LANES)
        slabs = lax.all_to_all(slabs, "ep", split_axis=0, concat_axis=0, tiled=True)
        return slabs.reshape(used * blocks, LANES)

    outputs = experts(used, exchange(send), pack, other)
    returned = exchange(outputs)
    give = combine(blocks // 2, False, returned, slots, parts, core)
    got = lax.ppermute(give, "tp", swap)
    keep = combine(blocks // 2, True, returned, slots, parts, core, resid)
    return (keep + got.astype(F32)).astype(BF16)


def solution(mesh):
    in_specs = (
        P("ep", None),
        P(),
        P(),
        P(None, "tp"),
        P(None, "tp"),
        P(None, "tp"),
        P(),
        P("tp", None),
        P("ep", None, "tp", None),
        P("ep", None, "tp", None),
        P("ep", "tp", None),
        P("ep"),
        P("ep", None),
        P("ep", None),
        P("ep", None, "tp"),
        P("ep", None, "tp"),
        P("ep", "tp", None),
    )
    out_specs = P("ep", "tp")
    return jax.shard_map(shards, mesh=mesh, in_specs=in_specs, out_specs=out_specs, check_vma=False)
```
